32 devices in a mesh: gr: 2 (over x), fs: 8 (over z, y), tp: 2 (over core).
Axes of the slice: x: 2, y: 2, z: 4, core: 2. Of those that a mesh axis runs over, the one named last changes fastest.
Arguments:
- tokens: bfloat16 [4096, 2048], P(('gr', 'fs', 'tp')), may hold values from -6 to 6
- routes: int32 [4096, 8], P(('gr', 'fs', 'tp')), may hold values from 0 to 15, all different within a row; in each aligned block of 128 rows (0 to 127, 128 to 255, ...) at most 96 rows name the same one
- route_weights: float32 [4096, 8], P(('gr', 'fs', 'tp')), may hold values from 0.1 to 0.6
- norm_gain: float32 [2048], P(('gr', 'tp')), may hold values from 0.1 to 1.9
- gate_trained: float32 [16, 384, 2048], P(None, 'fs', ('gr', 'tp')), may hold values from -0.125 to 0.125
- up_trained: float32 [16, 384, 2048], P(None, 'fs', ('gr', 'tp')), may hold values from -0.125 to 0.125
- down_trained: float32 [16, 384, 2048], P(None, 'fs', ('gr', 'tp')), may hold values from -0.3125 to 0.3125
- shared_gate_trained: float32 [512, 2048], P('fs', ('gr', 'tp')), may hold values from -0.125 to 0.125
- shared_up_trained: float32 [512, 2048], P('fs', ('gr', 'tp')), may hold values from -0.125 to 0.125
- shared_down_trained: float32 [512, 2048], P('fs', ('gr', 'tp')), may hold values from -0.25 to 0.25
Outputs:
- combined: bfloat16 [4096, 2048], P(('gr', 'fs', 'tp'))
- expert_gate: bfloat16 [16, 384, 2048], P(('fs', 'tp'))
- expert_up: bfloat16 [16, 384, 2048], P(('fs', 'tp'))
- expert_down: bfloat16 [16, 384, 2048], P(('fs', 'tp'))
- shared_gate: bfloat16 [512, 2048], P('fs')
- shared_up: bfloat16 [512, 2048], P('fs')
- shared_down: bfloat16 [512, 2048], P('fs')
The draws below stay inside these ranges and needn't reach their ends.
Inputs may be any that keep to these rules, and one draw needn't show every extreme that they name: `routes`: each row names 8 different experts. Among the rows of one device no expert is named more than 96 times, and that many is reached in every draw.
All inputs are finite; a program needn't handle non-finite values.
Results may differ from the reference program's by a relative error of at most 0.0084.
Values may be sent and summed in bfloat16 or wider, within the bound.
A program may use at most 128 MiB of HBM per device.

```python
import math
import jax
import jax.numpy as jnp
import numpy as np
from jax import lax

D = 2048
HE = 384
SH = 512
TOP_K = 8
TOK_DEV = 128
EXPERTS = 16
CAP = 96
TOKENS = 4096
N_GR = 2
N_FS = 8
N_TP = 2


def block_levels(rng, extent, split, smallest, largest):
    def one(axis_at, shards_of):
        steps = jax.random.uniform(jax.random.fold_in(jax.random.fold_in(rng, 6), axis_at), (shards_of,), jnp.float32, smallest / len(split), largest / len(split))
        return jnp.repeat(jnp.exp(steps), extent[axis_at] // shards_of).reshape((-1,) + (1,) * (len(extent) - axis_at - 1))

    factor_of = one(*split[0])
    for cut in split[1:]:
        factor_of = factor_of * one(*cut)
    return factor_of


def routed_block(key, own, number, rows, count, top, bound, lean):
    sequence = jax.random.permutation(key, count)
    crowded, common = shares(count, rows * top, bound, lean, True), shares(count, rows * top, bound, lean, False)
    places = jnp.arange(count)

    def named(tallies, turn):
        used = int((tallies > 0).sum())
        fixed = max(1, used // 4)
        passed = fixed + (places - fixed + turn * (used - fixed)) % max(1, count - fixed)
        return jnp.zeros((count,), jnp.int32).at[sequence[jnp.where(places < fixed, places, passed)]].set(jnp.asarray(tallies, jnp.int32))

    tallies = jnp.where(number % 4 == 0, named(crowded, number // 4), named(common, number - number // 4 - 1))
    mixed = jax.random.permutation(jax.random.fold_in(own, 3), count)
    source_of, receiver = mixed[0:count // 2 * 2:2], mixed[1:count // 2 * 2:2]
    margin = jnp.minimum(tallies[source_of] - 1, bound - tallies[receiver]) // 2
    margin = jnp.where((source_of == sequence[0]) | (receiver == sequence[0]) | (tallies[receiver] == 0), 0, jnp.maximum(margin, 0))
    passed = jax.random.randint(jax.random.fold_in(own, 4), (count // 2,), 0, 1 << 20) % (margin + 1)
    tallies = tallies.at[source_of].add(-passed).at[receiver].add(passed)
    members = jnp.searchsorted(jnp.cumsum(tallies), jnp.arange(rows * top), side="right").astype(jnp.int32)
    table = members.reshape(top, rows).T
    table = table[jax.random.permutation(jax.random.fold_in(own, 1), rows)]
    turn = jax.random.randint(jax.random.fold_in(own, 2), (rows, 1), 0, top)
    return jnp.take_along_axis(table, (jnp.arange(top)[None, :] + turn) % top, axis=1)


def shares(amount, total, most, lean, full):
    weights = [(1 << 20) // math.isqrt(rank ** lean) + 1 for rank in range(1, amount + 1)]
    largest = most if full else min(most, max(-(-total // amount), total * weights[0] // sum(weights)))
    least = 1 if total - largest >= amount - 1 else 0
    holding, rest = [largest] + [least] * (amount - 1), total - largest - least * (amount - 1)
    while rest > 0:
        candidates = [i for i in range(1, amount) if holding[i] < largest] or [i for i in range(1, amount) if holding[i] < most]
        pool, remaining = sum([weights[i] for i in candidates]), rest
        for i in candidates:
            more = min(most - holding[i], max(1, remaining * weights[i] // pool), rest)
            holding[i] = holding[i] + more
            rest = rest - more
    return np.array(holding)


def scatter_about(own_key, extent, scale, most, pieces=(), kind=jnp.bfloat16):
    drawn = jax.random.normal(own_key, extent, jnp.float32) * scale
    if len(pieces) > 0:
        drawn = block_levels(own_key, extent, pieces, -0.22, 0.18) * drawn
    return jnp.clip(drawn, min=-most, max=most).astype(kind)


def setup_inputs(seed: int = 0) -> dict:
    key_of = jax.random.split(jax.random.key(seed), 11)
    tokens = scatter_about(key_of[0], (TOKENS, D), 1.0, 6.0, ((0, 32),))
    routes_keys = jax.random.split(jax.random.fold_in(key_of[1], 1), TOKENS // TOK_DEV)
    routes_turns = jax.random.permutation(jax.random.fold_in(key_of[1], 3), TOKENS // TOK_DEV)
    routes = jax.vmap(lambda own, number: routed_block(jax.random.fold_in(key_of[1], 2), own, number, TOK_DEV, EXPERTS, TOP_K, CAP, 1))(routes_keys, routes_turns).reshape((TOKENS, TOP_K))
    route_weights = jnp.clip(0.1 + 0.5 * jax.random.uniform(key_of[2], (TOKENS, TOP_K), jnp.float32) ** block_levels(key_of[2], (TOKENS, TOP_K), ((0, 32),), -0.2, 0.2), 0.1, 0.6)
    norm_gain = jnp.clip(1.0 + 0.18 * jax.random.normal(key_of[3], (D,), jnp.float32), 0.1, 1.9)
    gate_trained = scatter_about(key_of[4], (EXPERTS, HE, D), D ** -0.5, 0.125, ((1, 8), (2, 4)), jnp.float32)
    up_trained = scatter_about(key_of[5], (EXPERTS, HE, D), D ** -0.5, 0.125, ((1, 8), (2, 4)), jnp.float32)
    down_trained = scatter_about(key_of[6], (EXPERTS, HE, D), HE ** -0.5, 0.3125, ((1, 8), (2, 4)), jnp.float32)
    shared_gate_trained = scatter_about(key_of[7], (SH, D), D ** -0.5, 0.125, ((0, 8), (1, 4)), jnp.float32)
    shared_up_trained = scatter_about(key_of[8], (SH, D), D ** -0.5, 0.125, ((0, 8), (1, 4)), jnp.float32)
    shared_down_trained = scatter_about(key_of[9], (SH, D), SH ** -0.5, 0.25, ((0, 8), (1, 4)), jnp.float32)
    return dict(tokens=tokens, routes=routes, route_weights=route_weights, norm_gain=norm_gain, gate_trained=gate_trained, up_trained=up_trained, down_trained=down_trained, shared_gate_trained=shared_gate_trained, shared_up_trained=shared_up_trained, shared_down_trained=shared_down_trained)


epsilon = 1e-06

def contract_rows(inputs, matrix):
    return lax.dot_general(inputs, matrix, (((1,), (1,)), ((), ())), preferred_element_type=jnp.float32)

def swiglu_rows(inputs, gate_matrix, up_matrix, down_matrix):
    hidden = (jax.nn.silu(contract_rows(inputs, gate_matrix)) * contract_rows(inputs, up_matrix)).astype(jnp.bfloat16)
    return jnp.dot(hidden, down_matrix, preferred_element_type=jnp.float32)

def reference(tokens, routes, route_weights, norm_gain, gate_trained, up_trained, down_trained, shared_gate_trained, shared_up_trained, shared_down_trained):
    expert_gate = (gate_trained * norm_gain[None, None, :]).astype(jnp.bfloat16)
    expert_up = (up_trained * norm_gain[None, None, :]).astype(jnp.bfloat16)
    expert_down = down_trained.astype(jnp.bfloat16)
    shared_gate = (shared_gate_trained * norm_gain[None, :]).astype(jnp.bfloat16)
    shared_up = (shared_up_trained * norm_gain[None, :]).astype(jnp.bfloat16)
    shared_down = shared_down_trained.astype(jnp.bfloat16)
    values = tokens.astype(jnp.float32)
    normed = (values * lax.rsqrt(lax.optimization_barrier(jnp.mean(values * values, axis=1, keepdims=True)) + epsilon)).astype(jnp.bfloat16)
    shared_out = swiglu_rows(normed, shared_gate, shared_up, shared_down)
    chosen = routes.reshape(-1).astype(jnp.int32)
    order = jnp.argsort(chosen, stable=True).astype(jnp.int32)
    sorted_tokens = (order // TOP_K).astype(jnp.int32)
    sorted_weights = route_weights.reshape(-1)[order]
    counts = jnp.bincount(chosen, length=EXPERTS).astype(jnp.int32)
    firsts = (jnp.cumsum(counts) - counts).astype(jnp.int32)
    limit = N_GR * N_FS * N_TP * CAP
    last_place = chosen.shape[0] - 1

    def per_expert(running, expert):
        offsets = jnp.arange(limit, dtype=jnp.int32)
        places = jnp.minimum(firsts[expert] + offsets, last_place).astype(jnp.int32)
        valid = offsets < counts[expert]
        rows_in = sorted_tokens[places]
        weights = jnp.where(valid, sorted_weights[places], jnp.zeros_like(sorted_weights[places]))
        result = swiglu_rows(normed[rows_in], expert_gate[expert], expert_up[expert], expert_down[expert]).astype(jnp.bfloat16)
        return (running.at[rows_in].add(weights[:, None] * result.astype(jnp.float32)), None)
    routed, _ = lax.scan(per_expert, jnp.zeros(tokens.shape, jnp.float32), jnp.arange(EXPERTS, dtype=jnp.int32))
    combined = (routed + shared_out).astype(jnp.bfloat16)
    return (combined, expert_gate, expert_up, expert_down, shared_gate, shared_up, shared_down)
```

```python
import functools

import jax
import jax.numpy as jnp
from jax import lax
from jax.experimental import pallas as pl
from jax.experimental.pallas import tpu as pltpu
from jax.sharding import PartitionSpec as P

epsilon = 1e-06
LANES = 128
MESH = pl.DeviceIdType.MESH


def contract_rows(inputs, matrix):
    return lax.dot_general(
        inputs, matrix, (((1,), (1,)), ((), ())), preferred_element_type=jnp.float32
    )


def swiglu_rows(inputs, gate_matrix, up_matrix, down_matrix):
    hidden = (
        jax.nn.silu(contract_rows(inputs, gate_matrix)) * contract_rows(inputs, up_matrix)
    ).astype(jnp.bfloat16)
    return jnp.dot(hidden, down_matrix, preferred_element_type=jnp.float32)


def dispatch_body(
    tokens,
    routes,
    route_weights,
    norm_gain,
    gate_trained,
    up_trained,
    down_trained,
    shared_gate_trained,
    shared_up_trained,
    shared_down_trained,
):
    gain_row = norm_gain[None, None, :]
    stacked = jnp.stack(
        [gate_trained * gain_row, up_trained * gain_row, down_trained], axis=1
    ).astype(jnp.bfloat16)
    halves = lax.all_to_all(
        lax.all_to_all(stacked[:, :, :, None, :], "fs", split_axis=0, concat_axis=2, tiled=True),
        "tp",
        split_axis=0,
        concat_axis=3,
        tiled=True,
    )
    owned = lax.all_gather(halves[:, :, :, None], "gr", axis=3, tiled=True)
    owned = owned.reshape(owned.shape[0], 3, owned.shape[2], -1)
    expert_gate = owned[:, 0]
    expert_up = owned[:, 1]
    expert_down = owned[:, 2]
    shared_gain = norm_gain[None, :]
    shared_stack = jnp.stack(
        [shared_gate_trained * shared_gain, shared_up_trained * shared_gain, shared_down_trained],
        axis=0,
    ).astype(jnp.bfloat16)
    shared_whole = lax.all_gather(shared_stack, ("gr", "tp"), axis=2, tiled=True)
    shared_gate = shared_whole[0]
    shared_up = shared_whole[1]
    shared_down = shared_whole[2]
    values = tokens.astype(jnp.float32)
    normed = (
        values * lax.rsqrt(jnp.mean(values * values, axis=1, keepdims=True) + epsilon)
    ).astype(jnp.bfloat16)
    row_count, features = normed.shape
    per_token = routes.shape[1]
    shared_out = swiglu_rows(
        normed,
        lax.all_gather(shared_gate, "fs", axis=0, tiled=True),
        lax.all_gather(shared_up, "fs", axis=0, tiled=True),
        lax.all_gather(shared_down, "fs", axis=0, tiled=True),
    )
    experts = lax.axis_size("fs") * lax.axis_size("tp")
    capacity = max(2, 3 * row_count * per_token // (2 * experts))
    chosen = routes.reshape(-1)
    onehot = (chosen[:, None] == jnp.arange(experts, dtype=jnp.int32)[None, :]).astype(jnp.int32)
    position = jnp.sum((jnp.cumsum(onehot, axis=0) - onehot) * onehot, axis=1)
    target = chosen * capacity + position
    source = (
        jnp.full((experts * capacity,), row_count, jnp.int32)
        .at[target]
        .set(jnp.arange(row_count * per_token, dtype=jnp.int32) // per_token)
    )
    padded = jnp.concatenate([normed, jnp.zeros((1, features), jnp.bfloat16)], axis=0)
    outgoing = padded[source].reshape(experts, capacity, features)
    arrived = lax.all_to_all(outgoing, ("fs", "tp"), split_axis=0, concat_axis=0, tiled=True)
    item_count = arrived.shape[1]
    result = swiglu_rows(
        arrived.reshape(-1, features), expert_gate[0], expert_up[0], expert_down[0]
    )
    result = result.astype(jnp.bfloat16).reshape(experts, item_count, features)
    returned = lax.all_to_all(result, ("fs", "tp"), split_axis=0, concat_axis=0, tiled=True)
    picked = returned.reshape(experts * capacity, features)[target].astype(jnp.float32)
    picked = picked.reshape(row_count, per_token, features)
    routed = jnp.sum(picked * route_weights[:, :, None], axis=1)
    combined = (routed + shared_out).astype(jnp.bfloat16)
    return (combined, expert_gate, expert_up, expert_down, shared_gate, shared_up, shared_down)


def exchange_kernel(
    n,
    pieces_ref,
    shared_ref,
    rows_ref,
    combined_ref,
    gate_ref,
    up_ref,
    down_ref,
    shared_gate_ref,
    shared_up_ref,
    shared_down_ref,
    weights,
    owned,
    shared,
    rows,
    select,
    parts,
    pair_in,
    sums,
    side_in,
    sums_in,
    local_sem,
    slice_out_sem,
    slice_sem,
    piece_sem,
    weight_sem,
    column_out_sem,
    column_sem,
    shared_out_sem,
    shared_sem,
    row_out_sem,
    row_side_sem,
    row_back_sem,
    row_sem,
    row_pair_out_sem,
    row_pair_sem,
    part_sem,
    part_recv_sem,
    side_sem,
    side_recv_sem,
    sum_sem,
    sum_recv_sem,
    out_sem,
):
    gr, fs, tp = lax.axis_index("gr"), lax.axis_index("fs"), lax.axis_index("tp")
    other = 1 - tp
    across = (1 - gr, fs, tp)
    across_twin = (1 - gr, fs, other)
    twin = (gr, fs, other)
    expert = fs * 2 + tp
    width = pieces_ref.shape[2]
    hidden_piece = pieces_ref.shape[1] // (2 * n)
    hidden = n * hidden_piece
    shared_piece = shared_ref.shape[1]
    extra = shared_piece // 2
    features = 4 * width
    row_count = rows_ref.shape[0]
    depth = n // 2
    outer, inner = lax.div(fs, 2), lax.rem(fs, 2)
    beside = (gr, outer * 2 + 1 - inner, tp)
    toward = jnp.where(outer < depth // 2, 1, -1)

    barrier = pltpu.get_barrier_semaphore()
    for device in (across, across_twin, twin):
        pl.semaphore_signal(barrier, inc=1, device_id=device, device_id_type=MESH)
    for k in range(1, n):
        for t in range(2):
            pl.semaphore_signal(
                barrier, inc=1, device_id=(gr, lax.rem(fs + k, n), t), device_id_type=MESH
            )
    pl.semaphore_wait(barrier, 2 * n + 1)

    def remote(src, dst, send, recv, device):
        return pltpu.make_async_remote_copy(
            src_ref=src,
            dst_ref=dst,
            send_sem=send,
            recv_sem=recv,
            device_id=device,
            device_id_type=MESH,
        )

    def columns(g, t):
        return pl.ds(pl.multiple_of((g * 2 + t) * width, width), width)

    def piece(e):
        return pieces_ref.at[:, pl.ds(pl.multiple_of(e * hidden_piece, 16), hidden_piece), :]

    def portion(t):
        return pieces_ref.at[:, pl.ds(pl.multiple_of(t * hidden, 16), hidden), :]

    def sliced(g, t):
        return weights.at[:, pl.ds(0, hidden), columns(g, t)]

    def slab(source, span):
        start = pl.multiple_of(source * hidden_piece, 16)
        return owned.at[:, pl.ds(start, hidden_piece), span]

    def row_block(source, t):
        start = pl.multiple_of((source * 2 + t) * row_count, row_count)
        return rows.at[pl.ds(start, row_count)]

    def nearby(k):
        place = lax.rem(outer + toward * lax.div(k, 2) + depth, depth)
        return place * 2 + jnp.where(lax.rem(k, 2) == 0, inner, 1 - inner)

    half = pl.ds(pl.multiple_of(gr * 2 * width, width), 2 * width)
    far_half = pl.ds(pl.multiple_of((1 - gr) * 2 * width, width), 2 * width)

    def slice_send(index, t, device):
        return remote(
            portion(t), sliced(gr, tp), slice_out_sem.at[index], slice_sem.at[index], device
        )

    def piece_send(d, t):
        return remote(
            piece(d * 2 + t),
            slab(fs, columns(gr, tp)),
            piece_sem.at[d, t],
            weight_sem.at[fs, tp],
            (gr, d, t),
        )

    def column_send(source):
        return remote(
            slab(source, half),
            slab(source, half),
            column_out_sem.at[source],
            column_sem.at[source],
            across,
        )

    def row_own(send, recv, device):
        return remote(rows_ref, row_block(fs, tp), send, recv, device)

    def row_move(source, send, recv, device):
        return remote(row_block(source, tp), row_block(source, tp), send, recv, device)

    def row_onward(source, step):
        return row_move(
            source,
            row_out_sem.at[source],
            row_sem.at[source],
            (gr, (outer + step) * 2 + inner, tp),
        )

    def row_beside(source):
        return row_move(source, row_side_sem.at[lax.div(source, 2)], row_sem.at[source], beside)

    def row_relay(source):
        return row_move(source, row_pair_out_sem.at[source], row_pair_sem.at[source], twin)

    own_up = row_own(row_out_sem.at[fs], row_sem.at[fs], (gr, (outer + 1) * 2 + inner, tp))
    own_back = row_own(row_back_sem.at[0], row_sem.at[fs], (gr, (outer - 1) * 2 + inner, tp))
    own_beside = row_own(row_side_sem.at[outer], row_sem.at[fs], beside)
    own_relay = row_own(row_pair_out_sem.at[fs], row_pair_sem.at[fs], twin)

    def at_distance(distance, action):
        for step in (1, -1):
            place = outer - step * distance

            @pl.when((place >= 0) & (place < depth))
            def _():
                action(place, step)

    def onward_exists(step):
        return (outer + step >= 0) & (outer + step < depth)

    @pl.when(outer < depth - 1)
    def _():
        own_up.start()

    @pl.when(outer > 0)
    def _():
        own_back.start()

    own_beside.start()
    shared_far = remote(
        shared_ref, shared.at[:, :, columns(gr, tp)], shared_out_sem.at[0], shared_sem.at[0], across
    )
    shared_far.start()
    slice_far = slice_send(0, tp, across)
    slice_cross = slice_send(1, other, across_twin)
    slice_twin = slice_send(2, other, twin)
    slice_far.start()
    slice_cross.start()
    own_relay.start()
    slice_twin.start()
    shared_twin = remote(
        shared_ref, shared.at[:, :, columns(gr, tp)], shared_out_sem.at[1], shared_sem.at[1], twin
    )
    shared_twin.start()
    twin_piece = piece_send(fs, other)
    twin_piece.start()

    def ship(step, distances):
        for distance in distances:
            place = outer + step * distance

            @pl.when((place >= 0) & (place < depth))
            def _():
                piece_send(place * 2 + inner, 0).start()
                piece_send(place * 2 + inner, 1).start()

    @pl.when(outer == 0)
    def _():
        ship(1, (1,))

    @pl.when(outer == depth - 1)
    def _():
        ship(-1, (1,))

    own_rows = pltpu.make_async_copy(rows_ref, row_block(fs, tp), local_sem.at[0])
    own_slice = pltpu.make_async_copy(portion(tp), sliced(gr, tp), local_sem.at[1])
    own_piece = pltpu.make_async_copy(piece(expert), slab(fs, columns(gr, tp)), local_sem.at[2])
    own_shared = pltpu.make_async_copy(
        shared_ref, shared.at[:, :, columns(gr, tp)], local_sem.at[3]
    )
    locals_ = (own_rows, own_slice, own_piece, own_shared)
    for copy in locals_:
        copy.start()
    lane = lax.broadcasted_iota(jnp.int32, select.shape, 0)
    unit = lax.broadcasted_iota(jnp.int32, select.shape, 1)
    first = (jnp.where(lane < LANES // 2, lane, lane - LANES // 2) - tp * n) * hidden_piece
    inside = (unit >= first) & (unit < first + hidden_piece) & (unit < hidden)
    select[...] = jnp.where(inside, 1.0, 0.0).astype(select.dtype)

    def take_rows(source):
        row_move(source, row_out_sem.at[source], row_sem.at[source], twin).wait_recv()

    def arrive(place, step):
        source = place * 2 + inner
        take_rows(source)

        @pl.when(onward_exists(step))
        def _():
            row_onward(source, step).start()

        row_beside(source).start()
        row_relay(source).start()

        @pl.when(place == (0 if step == 1 else depth - 1))
        def _():
            ship(step, range(1, depth))

    def arrive_beside(place, step):
        source = place * 2 + 1 - inner
        take_rows(source)
        row_relay(source).start()

    at_distance(1, arrive)
    for copy in locals_:
        copy.wait()
    far_columns = shared.at[:, :, columns(1 - gr, tp)]
    remote(shared_ref, far_columns, shared_out_sem.at[0], shared_sem.at[0], across).wait_recv()
    shared_relay = remote(far_columns, far_columns, shared_out_sem.at[2], shared_sem.at[2], twin)
    shared_relay.start()
    arrive_beside(outer, 0)
    for distance in range(2, depth):
        at_distance(distance, arrive)
        if distance == 2:

            @pl.when(outer == 0)
            def _():
                ship(1, range(2, depth))

            @pl.when(outer == depth - 1)
            def _():
                ship(-1, range(2, depth))

        at_distance(distance - 1, arrive_beside)

    for k in range(1, n, 2):
        d = nearby(k)
        piece_send(d, 0).start()
        piece_send(d, 1).start()

    def take_twin_piece(source, t):
        remote(
            piece(0),
            slab(source, columns(gr, t)),
            piece_sem.at[fs, other],
            weight_sem.at[source, t],
            twin,
        ).wait_recv()

    take_twin_piece(fs, other)
    column_send(fs).start()

    remote(
        shared_ref, shared.at[:, :, columns(gr, other)], shared_out_sem.at[1], shared_sem.at[1], twin
    ).wait_recv()
    last_columns = shared.at[:, :, columns(1 - gr, other)]
    remote(shared_ref, last_columns, shared_out_sem.at[2], shared_sem.at[2], twin).wait_recv()
    outs = []
    for j, ref in enumerate((shared_gate_ref, shared_up_ref, shared_down_ref)):
        outs.append(pltpu.make_async_copy(shared.at[j], ref, out_sem.at[3 + j]))
    for copy in outs:
        copy.start()
    tail = pltpu.make_async_copy(
        shared.at[:, pl.ds(pl.multiple_of(tp * extra, extra), extra), :],
        weights.at[:, pl.ds(hidden, extra), :],
        local_sem.at[4],
    )
    tail.start()
    tail.wait()
    remote(portion(tp), sliced(gr, other), slice_out_sem.at[2], slice_sem.at[2], twin).wait_recv()
    remote(portion(tp), sliced(1 - gr, tp), slice_out_sem.at[0], slice_sem.at[0], across).wait_recv()
    remote(
        portion(tp), sliced(1 - gr, other), slice_out_sem.at[1], slice_sem.at[1], across
    ).wait_recv()

    def part_send(k):
        return remote(
            parts.at[k, pl.ds(pl.multiple_of(other * row_count, row_count), row_count), :],
            pair_in.at[k],
            part_sem.at[k],
            part_recv_sem.at[k],
            twin,
        )

    def place_of(j):
        return lax.rem(outer + toward * (j + 1) + depth, depth)

    def side_send(j):
        return remote(
            sums.at[2 * j], side_in.at[j], side_sem.at[j], side_recv_sem.at[j], beside
        )

    def sum_send(j):
        place = place_of(j)
        slot = lax.rem(outer - place + 2 * depth - 1, depth)
        return remote(
            sums.at[2 * j + 1],
            sums_in.at[slot],
            sum_sem.at[j],
            sum_recv_sem.at[slot],
            (gr, place * 2 + inner, tp),
        )

    chunk = 32

    def add_pair(k):
        part_send(k).wait_recv()

        @pl.loop(0, row_count // chunk)
        def _(i):
            at = pl.multiple_of(i * chunk, chunk)
            mine = pl.multiple_of(tp * row_count + i * chunk, chunk)
            value = parts[k, pl.ds(mine, chunk), :].astype(jnp.float32)
            value = value + pair_in[k, pl.ds(at, chunk), :].astype(jnp.float32)
            sums[k, pl.ds(at, chunk), :] = value.astype(jnp.bfloat16)

    def add_both(j):
        k = 2 * j + 1
        part_send(k).wait_recv()
        side_send(j).wait_recv()

        @pl.loop(0, row_count // chunk)
        def _(i):
            at = pl.multiple_of(i * chunk, chunk)
            mine = pl.multiple_of(tp * row_count + i * chunk, chunk)
            value = parts[k, pl.ds(mine, chunk), :].astype(jnp.float32)
            value = value + pair_in[k, pl.ds(at, chunk), :].astype(jnp.float32)
            value = value + side_in[j, pl.ds(at, chunk), :].astype(jnp.float32)
            sums[k, pl.ds(at, chunk), :] = value.astype(jnp.bfloat16)

    def take_weights(source):
        take_twin_piece(source, 0)
        take_twin_piece(source, 1)
        column_send(source).start()

    @pl.loop(0, n)
    def _(k):
        j = lax.div(k, 2)
        d = place_of(j) * 2 + jnp.where(lax.rem(k, 2) == 0, 1 - inner, inner)

        @pl.when(k == n - 4)
        def _():
            at_distance(depth - 1, arrive_beside)

        remote(
            row_block(d, other), row_block(d, other), row_pair_out_sem.at[d], row_pair_sem.at[d], twin
        ).wait_recv()
        block = pl.ds(pl.multiple_of(d * 2 * row_count, 2 * row_count), 2 * row_count)
        inputs = rows[block, 0:features]
        scale = jnp.dot(
            rows[block, features : features + LANES],
            select[...],
            preferred_element_type=jnp.float32,
        )
        gate = contract_rows(inputs, weights[0])
        up = contract_rows(inputs, weights[1])
        position = lax.broadcasted_iota(jnp.int32, gate.shape, 1)
        scale = jnp.where(position < hidden, scale, 1.0)
        units = (gate / (1.0 + jnp.exp(-gate)) * up * scale).astype(jnp.bfloat16)
        for c in range(4):
            span = pl.ds(c * width, width)
            parts[k, :, span] = jnp.dot(
                units, weights[2, :, span], preferred_element_type=jnp.float32
            ).astype(jnp.bfloat16)
        part_send(k).start()

        @pl.when(lax.rem(k, 2) == 1)
        def _():
            add_pair(k - 1)
            side_send(j).start()

        @pl.when((k > 0) & (k < depth))
        def _():
            take_weights(nearby(2 * k))

    take_weights(nearby(1))
    for j in range(depth - 1):
        take_weights(nearby(2 * j + 3))
        add_both(j)
        sum_send(j).start()

    for k in range(n):
        source = nearby(k)
        remote(
            slab(source, far_half),
            slab(source, far_half),
            column_out_sem.at[source],
            column_sem.at[source],
            across,
        ).wait_recv()
    for j, ref in enumerate((gate_ref, up_ref, down_ref)):
        copy = pltpu.make_async_copy(owned.at[j], ref.at[0], out_sem.at[j])
        copy.start()
        outs.append(copy)

    add_both(depth - 1)
    for j in range(depth - 1):
        remote(sums.at[0], sums_in.at[j], sum_sem.at[j], sum_recv_sem.at[j], twin).wait_recv()

    @pl.loop(0, row_count // chunk)
    def _(i):
        at = pl.ds(pl.multiple_of(i * chunk, chunk), chunk)
        total = sums[n - 1, at, :].astype(jnp.float32)
        for j in range(depth - 1):
            total = total + sums_in[j, at, :].astype(jnp.float32)
        combined_ref[at, :] = total.astype(jnp.bfloat16)

    @pl.when(outer < depth - 1)
    def _():
        own_up.wait_send()

    @pl.when(outer > 0)
    def _():
        own_back.wait_send()

    for copy in (
        own_beside,
        own_relay,
        shared_far,
        slice_far,
        slice_cross,
        slice_twin,
        shared_twin,
        twin_piece,
        shared_relay,
    ):
        copy.wait_send()

    def sent(place, step):
        source = place * 2 + inner

        @pl.when(onward_exists(step))
        def _():
            row_onward(source, step).wait_send()

        row_beside(source).wait_send()

    for distance in range(1, depth):
        at_distance(distance, sent)
    column_send(fs).wait_send()
    for k in range(1, n):
        d = lax.rem(fs + k, n)
        piece_send(d, 0).wait_send()
        piece_send(d, 1).wait_send()
        column_send(d).wait_send()
        row_relay(d).wait_send()
    for k in range(n):
        part_send(k).wait_send()
    for j in range(depth):
        side_send(j).wait_send()
    for j in range(depth - 1):
        sum_send(j).wait_send()
    for copy in outs:
        copy.wait()


def direct_body(
    tokens,
    routes,
    route_weights,
    norm_gain,
    gate_trained,
    up_trained,
    down_trained,
    shared_gate_trained,
    shared_up_trained,
    shared_down_trained,
):
    gain_row = norm_gain[None, None, :]
    experts, hidden_piece, width = gate_trained.shape
    pieces = (
        jnp.stack([gate_trained * gain_row, up_trained * gain_row, down_trained], axis=0)
        .astype(jnp.bfloat16)
        .reshape(3, experts * hidden_piece, width)
    )
    shared_gain = norm_gain[None, :]
    shared_stack = jnp.stack(
        [shared_gate_trained * shared_gain, shared_up_trained * shared_gain, shared_down_trained],
        axis=0,
    ).astype(jnp.bfloat16)
    values = tokens.astype(jnp.float32)
    normed = (
        values * lax.rsqrt(jnp.mean(values * values, axis=1, keepdims=True) + epsilon)
    ).astype(jnp.bfloat16)
    n = lax.axis_size("fs")
    row_count, features = normed.shape
    shared_piece = shared_stack.shape[1]
    numbers = jnp.arange(LANES // 2, dtype=jnp.int32)
    factors = jnp.sum(
        jnp.where(routes[:, :, None] == numbers, route_weights[:, :, None], 0.0), axis=1
    )
    high = lax.reduce_precision(factors, 8, 7)
    rows = jnp.concatenate(
        [normed, high.astype(jnp.bfloat16), (factors - high).astype(jnp.bfloat16)], axis=1
    )
    hidden = n * hidden_piece
    hidden_all = hidden + shared_piece // 2
    vmem = pl.BlockSpec(memory_space=pltpu.VMEM)
    hbm = pl.BlockSpec(memory_space=pl.ANY)
    kind = jnp.bfloat16
    expert_shape = jax.ShapeDtypeStruct((1, hidden, features), kind)
    shared_shape = jax.ShapeDtypeStruct((shared_piece, features), kind)
    DMA = pltpu.SemaphoreType.DMA
    return pl.pallas_call(
        functools.partial(exchange_kernel, n),
        out_shape=(jax.ShapeDtypeStruct((row_count, features), kind),)
        + (expert_shape,) * 3
        + (shared_shape,) * 3,
        in_specs=[vmem] * 3,
        out_specs=(vmem,) + (hbm,) * 6,
        scratch_shapes=[
            pltpu.VMEM((3, hidden_all, features), kind),
            pltpu.VMEM((3, hidden, features), kind),
            pltpu.VMEM((3, shared_piece, features), kind),
            pltpu.VMEM((experts * row_count, features + LANES), kind),
            pltpu.VMEM((LANES, hidden_all), kind),
            pltpu.VMEM((n, 2 * row_count, features), kind),
            pltpu.VMEM((n, row_count, features), kind),
            pltpu.VMEM((n, row_count, features), kind),
            pltpu.VMEM((n // 2, row_count, features), kind),
            pltpu.VMEM((n // 2 - 1, row_count, features), kind),
            DMA((5,)),
            DMA((3,)),
            DMA((3,)),
            DMA((n, 2)),
            DMA((n, 2)),
            DMA((n,)),
            DMA((n,)),
            DMA((3,)),
            DMA((3,)),
            DMA((n,)),
            DMA((n // 2,)),
            DMA((1,)),
            DMA((n,)),
            DMA((n,)),
            DMA((n,)),
            DMA((n,)),
            DMA((n,)),
            DMA((n // 2,)),
            DMA((n // 2,)),
            DMA((n // 2 - 1,)),
            DMA((n // 2 - 1,)),
            DMA((6,)),
        ],
        compiler_params=pltpu.CompilerParams(
            collective_id=0, has_side_effects=True, vmem_limit_bytes=60 * 1024 * 1024
        ),
    )(pieces, shared_stack, rows)


def body(*arguments):
    experts = lax.axis_size("fs") * lax.axis_size("tp")
    per_token = arguments[1].shape[1]
    pairs = lax.axis_size("gr") == 2 and lax.axis_size("tp") == 2
    if pairs and lax.axis_size("fs") % 2 == 0 and experts <= min(2 * per_token, LANES // 2):
        return direct_body(*arguments)
    return dispatch_body(*arguments)


def solution(mesh):
    in_specs = (
        P(("gr", "fs", "tp"), None),
        P(("gr", "fs", "tp"), None),
        P(("gr", "fs", "tp"), None),
        P(("gr", "tp")),
        P(None, "fs", ("gr", "tp")),
        P(None, "fs", ("gr", "tp")),
        P(None, "fs", ("gr", "tp")),
        P("fs", ("gr", "tp")),
        P("fs", ("gr", "tp")),
        P("fs", ("gr", "tp")),
    )
    out_specs = (
        P(("gr", "fs", "tp"), None),
        P(("fs", "tp"), None, None),
        P(("fs", "tp"), None, None),
        P(("fs", "tp"), None, None),
        P("fs", None),
        P("fs", None),
        P("fs", None),
    )
    return jax.shard_map(body, mesh=mesh, in_specs=in_specs, out_specs=out_specs, check_vma=False)
```

```python
import functools

import jax
import jax.numpy as jnp
from jax import lax
from jax.experimental import pallas as pl
from jax.experimental.pallas import tpu as pltpu
from jax.sharding import PartitionSpec as P

epsilon = 1e-06
LANES = 128
MESH = pl.DeviceIdType.MESH


def contract_rows(inputs, matrix):
    return lax.dot_general(
        inputs, matrix, (((1,), (1,)), ((), ())), preferred_element_type=jnp.float32
    )


def swiglu_rows(inputs, gate_matrix, up_matrix, down_matrix):
    hidden = (
        jax.nn.silu(contract_rows(inputs, gate_matrix)) * contract_rows(inputs, up_matrix)
    ).astype(jnp.bfloat16)
    return jnp.dot(hidden, down_matrix, preferred_element_type=jnp.float32)


def dispatch_body(
    tokens,
    routes,
    route_weights,
    norm_gain,
    gate_trained,
    up_trained,
    down_trained,
    shared_gate_trained,
    shared_up_trained,
    shared_down_trained,
):
    gain_row = norm_gain[None, None, :]
    stacked = jnp.stack(
        [gate_trained * gain_row, up_trained * gain_row, down_trained], axis=1
    ).astype(jnp.bfloat16)
    halves = lax.all_to_all(
        lax.all_to_all(stacked[:, :, :, None, :], "fs", split_axis=0, concat_axis=2, tiled=True),
        "tp",
        split_axis=0,
        concat_axis=3,
        tiled=True,
    )
    owned = lax.all_gather(halves[:, :, :, None], "gr", axis=3, tiled=True)
    owned = owned.reshape(owned.shape[0], 3, owned.shape[2], -1)
    expert_gate = owned[:, 0]
    expert_up = owned[:, 1]
    expert_down = owned[:, 2]
    shared_gain = norm_gain[None, :]
    shared_stack = jnp.stack(
        [shared_gate_trained * shared_gain, shared_up_trained * shared_gain, shared_down_trained],
        axis=0,
    ).astype(jnp.bfloat16)
    shared_whole = lax.all_gather(shared_stack, ("gr", "tp"), axis=2, tiled=True)
    shared_gate = shared_whole[0]
    shared_up = shared_whole[1]
    shared_down = shared_whole[2]
    values = tokens.astype(jnp.float32)
    normed = (
        values * lax.rsqrt(jnp.mean(values * values, axis=1, keepdims=True) + epsilon)
    ).astype(jnp.bfloat16)
    row_count, features = normed.shape
    per_token = routes.shape[1]
    shared_out = swiglu_rows(
        normed,
        lax.all_gather(shared_gate, "fs", axis=0, tiled=True),
        lax.all_gather(shared_up, "fs", axis=0, tiled=True),
        lax.all_gather(shared_down, "fs", axis=0, tiled=True),
    )
    experts = lax.axis_size("fs") * lax.axis_size("tp")
    capacity = max(2, 3 * row_count * per_token // (2 * experts))
    chosen = routes.reshape(-1)
    onehot = (chosen[:, None] == jnp.arange(experts, dtype=jnp.int32)[None, :]).astype(jnp.int32)
    position = jnp.sum((jnp.cumsum(onehot, axis=0) - onehot) * onehot, axis=1)
    target = chosen * capacity + position
    source = (
        jnp.full((experts * capacity,), row_count, jnp.int32)
        .at[target]
        .set(jnp.arange(row_count * per_token, dtype=jnp.int32) // per_token)
    )
    padded = jnp.concatenate([normed, jnp.zeros((1, features), jnp.bfloat16)], axis=0)
    outgoing = padded[source].reshape(experts, capacity, features)
    arrived = lax.all_to_all(outgoing, ("fs", "tp"), split_axis=0, concat_axis=0, tiled=True)
    item_count = arrived.shape[1]
    result = swiglu_rows(
        arrived.reshape(-1, features), expert_gate[0], expert_up[0], expert_down[0]
    )
    result = result.astype(jnp.bfloat16).reshape(experts, item_count, features)
    returned = lax.all_to_all(result, ("fs", "tp"), split_axis=0, concat_axis=0, tiled=True)
    picked = returned.reshape(experts * capacity, features)[target].astype(jnp.float32)
    picked = picked.reshape(row_count, per_token, features)
    routed = jnp.sum(picked * route_weights[:, :, None], axis=1)
    combined = (routed + shared_out).astype(jnp.bfloat16)
    return (combined, expert_gate, expert_up, expert_down, shared_gate, shared_up, shared_down)


def exchange_kernel(
    n,
    tokens_hbm,
    routes_hbm,
    route_weights_hbm,
    gain_hbm,
    gate_hbm,
    up_hbm,
    down_hbm,
    shared_gate_hbm,
    shared_up_hbm,
    shared_down_hbm,
    combined_ref,
    owned,
    shared,
    weights,
    rows,
    select,
    tokens_ref,
    routes_ref,
    route_weights_ref,
    gain_ref,
    shared_stage,
    stage,
    pieces,
    shared_mine,
    parts,
    pair_in,
    sums,
    side_in,
    sums_in,
    local_sem,
    slice_out_sem,
    slice_sem,
    piece_sem,
    weight_sem,
    column_out_sem,
    column_sem,
    shared_out_sem,
    shared_sem,
    row_out_sem,
    row_side_sem,
    row_back_sem,
    row_sem,
    row_pair_out_sem,
    row_pair_sem,
    part_sem,
    part_recv_sem,
    side_sem,
    side_recv_sem,
    sum_sem,
    sum_recv_sem,
    stage_sem,
    input_sem,
):
    gr, fs, tp = lax.axis_index("gr"), lax.axis_index("fs"), lax.axis_index("tp")
    other = 1 - tp
    across = (1 - gr, fs, tp)
    across_twin = (1 - gr, fs, other)
    twin = (gr, fs, other)
    expert = fs * 2 + tp
    width = pieces.shape[2]
    hidden_piece = pieces.shape[1] // (2 * n)
    hidden = n * hidden_piece
    shared_piece = shared_mine.shape[1]
    extra = shared_piece // 2
    features = 4 * width
    row_count = tokens_ref.shape[0]
    depth = n // 2
    outer, inner = lax.div(fs, 2), lax.rem(fs, 2)
    beside = (gr, outer * 2 + 1 - inner, tp)
    toward = jnp.where(outer < depth // 2, 1, -1)

    inputs_in = []
    for i, (source, target) in enumerate(
        (
            (tokens_hbm, tokens_ref),
            (routes_hbm, routes_ref),
            (route_weights_hbm, route_weights_ref),
            (gain_hbm, gain_ref),
            (shared_gate_hbm, shared_stage.at[0]),
            (shared_up_hbm, shared_stage.at[1]),
            (shared_down_hbm, shared_stage.at[2]),
        )
    ):
        inputs_in.append(pltpu.make_async_copy(source, target, input_sem.at[i]))
        inputs_in[i].start()
    staged = {}
    for t in (0, 1):
        for j, ref in enumerate((gate_hbm, up_hbm, down_hbm)):
            part = pl.ds(t * hidden, hidden)
            staged[j, t] = pltpu.make_async_copy(ref.at[part], stage.at[j, part], stage_sem.at[j, t])
            staged[j, t].start()

    barrier = pltpu.get_barrier_semaphore()
    for device in (across, across_twin, twin):
        pl.semaphore_signal(barrier, inc=1, device_id=device, device_id_type=MESH)
    for k in range(1, n):
        for t in range(2):
            pl.semaphore_signal(
                barrier, inc=1, device_id=(gr, lax.rem(fs + k, n), t), device_id_type=MESH
            )

    own_start = pl.multiple_of(expert * row_count, row_count)
    few = 16
    for copy in inputs_in:
        copy.wait()

    @pl.loop(0, row_count // few)
    def _(i):
        at = pl.multiple_of(i * few, few)
        values = tokens_ref[pl.ds(at, few), :].astype(jnp.float32)
        mean = jnp.mean(values * values, axis=1, keepdims=True)
        normed = (values * lax.rsqrt(mean + epsilon)).astype(jnp.bfloat16)
        rows[pl.ds(own_start + at, few), 0:features] = normed

    number = lax.broadcasted_iota(jnp.int32, (LANES // 2, row_count), 0)
    factors = jnp.zeros(number.shape, jnp.float32)
    for k in range(routes_ref.shape[0]):
        named = routes_ref[k : k + 1, :] == number
        factors = factors + jnp.where(named, route_weights_ref[k : k + 1, :], 0.0)
    high = factors.astype(jnp.bfloat16).astype(jnp.float32)
    both = jnp.concatenate([high, factors - high], axis=0)
    rows[pl.ds(own_start, row_count), features : features + LANES] = both.T.astype(jnp.bfloat16)

    gain = gain_ref[...]
    for j in range(3):
        value = shared_stage[j] if j == 2 else shared_stage[j] * gain
        shared_mine[j] = value.astype(jnp.bfloat16)
    for t in (0, 1):
        for j in range(3):
            staged[j, t].wait()

            @pl.loop(0, n)
            def _(i):
                at = pl.ds(pl.multiple_of((t * n + i) * hidden_piece, hidden_piece), hidden_piece)
                value = stage[j, at, :] if j == 2 else stage[j, at, :] * gain_ref[...]
                pieces[j, at, :] = value.astype(jnp.bfloat16)

    lane = lax.broadcasted_iota(jnp.int32, select.shape, 0)
    unit = lax.broadcasted_iota(jnp.int32, select.shape, 1)
    first = (jnp.where(lane < LANES // 2, lane, lane - LANES // 2) - tp * n) * hidden_piece
    inside = (unit >= first) & (unit < first + hidden_piece) & (unit < hidden)
    select[...] = jnp.where(inside, 1.0, 0.0).astype(select.dtype)
    pl.semaphore_wait(barrier, 2 * n + 1)

    def remote(src, dst, send, recv, device):
        return pltpu.make_async_remote_copy(
            src_ref=src,
            dst_ref=dst,
            send_sem=send,
            recv_sem=recv,
            device_id=device,
            device_id_type=MESH,
        )

    def columns(g, t):
        return pl.ds(pl.multiple_of((g * 2 + t) * width, width), width)

    def piece(e):
        return pieces.at[:, pl.ds(pl.multiple_of(e * hidden_piece, 16), hidden_piece), :]

    def portion(t):
        return pieces.at[:, pl.ds(pl.multiple_of(t * hidden, 16), hidden), :]

    def sliced(g, t):
        return weights.at[:, pl.ds(0, hidden), columns(g, t)]

    def slab(source, span):
        start = pl.multiple_of(source * hidden_piece, 16)
        return owned.at[:, pl.ds(start, hidden_piece), span]

    def row_block(source, t):
        start = pl.multiple_of((source * 2 + t) * row_count, row_count)
        return rows.at[pl.ds(start, row_count)]

    def nearby(k):
        place = lax.rem(outer + toward * lax.div(k, 2) + depth, depth)
        return place * 2 + jnp.where(lax.rem(k, 2) == 0, inner, 1 - inner)

    half = pl.ds(pl.multiple_of(gr * 2 * width, width), 2 * width)
    far_half = pl.ds(pl.multiple_of((1 - gr) * 2 * width, width), 2 * width)

    def slice_send(index, t, device):
        return remote(
            portion(t), sliced(gr, tp), slice_out_sem.at[index], slice_sem.at[index], device
        )

    def piece_send(d, t):
        return remote(
            piece(d * 2 + t),
            slab(fs, columns(gr, tp)),
            piece_sem.at[d, t],
            weight_sem.at[fs, tp],
            (gr, d, t),
        )

    def column_send(source):
        return remote(
            slab(source, half),
            slab(source, half),
            column_out_sem.at[source],
            column_sem.at[source],
            across,
        )

    def row_move(source, send, recv, device):
        return remote(row_block(source, tp), row_block(source, tp), send, recv, device)

    def row_onward(source, step):
        return row_move(
            source,
            row_out_sem.at[source],
            row_sem.at[source],
            (gr, (outer + step) * 2 + inner, tp),
        )

    def row_beside(source):
        return row_move(source, row_side_sem.at[lax.div(source, 2)], row_sem.at[source], beside)

    def row_relay(source):
        return row_move(source, row_pair_out_sem.at[source], row_pair_sem.at[source], twin)

    own_up = row_move(fs, row_out_sem.at[fs], row_sem.at[fs], (gr, (outer + 1) * 2 + inner, tp))
    own_back = row_move(fs, row_back_sem.at[0], row_sem.at[fs], (gr, (outer - 1) * 2 + inner, tp))
    own_beside = row_move(fs, row_side_sem.at[outer], row_sem.at[fs], beside)
    own_relay = row_move(fs, row_pair_out_sem.at[fs], row_pair_sem.at[fs], twin)

    def at_distance(distance, action):
        for step in (1, -1):
            place = outer - step * distance

            @pl.when((place >= 0) & (place < depth))
            def _():
                action(place, step)

    def onward_exists(step):
        return (outer + step >= 0) & (outer + step < depth)

    @pl.when(outer < depth - 1)
    def _():
        own_up.start()

    @pl.when(outer > 0)
    def _():
        own_back.start()

    own_beside.start()
    shared_far = remote(
        shared_mine, shared.at[:, :, columns(gr, tp)], shared_out_sem.at[0], shared_sem.at[0], across
    )
    shared_far.start()
    slice_far = slice_send(0, tp, across)
    slice_cross = slice_send(1, other, across_twin)
    slice_twin = slice_send(2, other, twin)
    slice_far.start()
    slice_cross.start()
    own_relay.start()
    slice_twin.start()
    shared_twin = remote(
        shared_mine, shared.at[:, :, columns(gr, tp)], shared_out_sem.at[1], shared_sem.at[1], twin
    )
    shared_twin.start()
    twin_piece = piece_send(fs, other)
    twin_piece.start()

    def ship(step, distances):
        for distance in distances:
            place = outer + step * distance

            @pl.when((place >= 0) & (place < depth))
            def _():
                piece_send(place * 2 + inner, 0).start()
                piece_send(place * 2 + inner, 1).start()

    @pl.when(outer == 0)
    def _():
        ship(1, (1,))

    @pl.when(outer == depth - 1)
    def _():
        ship(-1, (1,))

    own_slice = pltpu.make_async_copy(portion(tp), sliced(gr, tp), local_sem.at[1])
    own_piece = pltpu.make_async_copy(piece(expert), slab(fs, columns(gr, tp)), local_sem.at[2])
    own_shared = pltpu.make_async_copy(
        shared_mine, shared.at[:, :, columns(gr, tp)], local_sem.at[3]
    )
    locals_ = (own_slice, own_piece, own_shared)
    for copy in locals_:
        copy.start()

    def take_rows(source):
        row_move(source, row_out_sem.at[source], row_sem.at[source], twin).wait_recv()

    def arrive(place, step):
        source = place * 2 + inner
        take_rows(source)

        @pl.when(onward_exists(step))
        def _():
            row_onward(source, step).start()

        row_beside(source).start()
        row_relay(source).start()

        @pl.when(place == (0 if step == 1 else depth - 1))
        def _():
            ship(step, range(1, depth))

    def arrive_beside(place, step):
        source = place * 2 + 1 - inner
        take_rows(source)
        row_relay(source).start()

    at_distance(1, arrive)
    for copy in locals_:
        copy.wait()
    far_columns = shared.at[:, :, columns(1 - gr, tp)]
    remote(shared_mine, far_columns, shared_out_sem.at[0], shared_sem.at[0], across).wait_recv()
    shared_relay = remote(far_columns, far_columns, shared_out_sem.at[2], shared_sem.at[2], twin)
    shared_relay.start()
    arrive_beside(outer, 0)
    for distance in range(2, depth):
        at_distance(distance, arrive)
        if distance == 2:

            @pl.when(outer == 0)
            def _():
                ship(1, range(2, depth))

            @pl.when(outer == depth - 1)
            def _():
                ship(-1, range(2, depth))

        at_distance(distance - 1, arrive_beside)

    for k in range(1, n, 2):
        d = nearby(k)
        piece_send(d, 0).start()
        piece_send(d, 1).start()

    def take_twin_piece(source, t):
        remote(
            piece(0),
            slab(source, columns(gr, t)),
            piece_sem.at[fs, other],
            weight_sem.at[source, t],
            twin,
        ).wait_recv()

    take_twin_piece(fs, other)
    column_send(fs).start()

    remote(
        shared_mine, shared.at[:, :, columns(gr, other)], shared_out_sem.at[1], shared_sem.at[1], twin
    ).wait_recv()
    last_columns = shared.at[:, :, columns(1 - gr, other)]
    remote(shared_mine, last_columns, shared_out_sem.at[2], shared_sem.at[2], twin).wait_recv()
    tail = pltpu.make_async_copy(
        shared.at[:, pl.ds(pl.multiple_of(tp * extra, extra), extra), :],
        weights.at[:, pl.ds(hidden, extra), :],
        local_sem.at[4],
    )
    tail.start()
    tail.wait()
    remote(portion(tp), sliced(gr, other), slice_out_sem.at[2], slice_sem.at[2], twin).wait_recv()
    remote(portion(tp), sliced(1 - gr, tp), slice_out_sem.at[0], slice_sem.at[0], across).wait_recv()
    remote(
        portion(tp), sliced(1 - gr, other), slice_out_sem.at[1], slice_sem.at[1], across
    ).wait_recv()

    def part_send(k):
        return remote(
            parts.at[k, pl.ds(pl.multiple_of(other * row_count, row_count), row_count), :],
            pair_in.at[k],
            part_sem.at[k],
            part_recv_sem.at[k],
            twin,
        )

    def place_of(j):
        return lax.rem(outer + toward * (j + 1) + depth, depth)

    def side_send(j):
        return remote(
            sums.at[2 * j], side_in.at[j], side_sem.at[j], side_recv_sem.at[j], beside
        )

    def sum_send(j):
        place = place_of(j)
        slot = lax.rem(outer - place + 2 * depth - 1, depth)
        return remote(
            sums.at[2 * j + 1],
            sums_in.at[slot],
            sum_sem.at[j],
            sum_recv_sem.at[slot],
            (gr, place * 2 + inner, tp),
        )

    chunk = 32

    def add_pair(k):
        part_send(k).wait_recv()

        @pl.loop(0, row_count // chunk)
        def _(i):
            at = pl.multiple_of(i * chunk, chunk)
            mine = pl.multiple_of(tp * row_count + i * chunk, chunk)
            value = parts[k, pl.ds(mine, chunk), :].astype(jnp.float32)
            value = value + pair_in[k, pl.ds(at, chunk), :].astype(jnp.float32)
            sums[k, pl.ds(at, chunk), :] = value.astype(jnp.bfloat16)

    def add_both(j):
        k = 2 * j + 1
        part_send(k).wait_recv()
        side_send(j).wait_recv()

        @pl.loop(0, row_count // chunk)
        def _(i):
            at = pl.multiple_of(i * chunk, chunk)
            mine = pl.multiple_of(tp * row_count + i * chunk, chunk)
            value = parts[k, pl.ds(mine, chunk), :].astype(jnp.float32)
            value = value + pair_in[k, pl.ds(at, chunk), :].astype(jnp.float32)
            value = value + side_in[j, pl.ds(at, chunk), :].astype(jnp.float32)
            sums[k, pl.ds(at, chunk), :] = value.astype(jnp.bfloat16)

    def take_weights(source):
        take_twin_piece(source, 0)
        take_twin_piece(source, 1)
        column_send(source).start()

    @pl.loop(0, n)
    def _(k):
        j = lax.div(k, 2)
        d = place_of(j) * 2 + jnp.where(lax.rem(k, 2) == 0, 1 - inner, inner)

        @pl.when(k == n - 4)
        def _():
            at_distance(depth - 1, arrive_beside)

        remote(
            row_block(d, other), row_block(d, other), row_pair_out_sem.at[d], row_pair_sem.at[d], twin
        ).wait_recv()
        block = pl.ds(pl.multiple_of(d * 2 * row_count, 2 * row_count), 2 * row_count)
        inputs = rows[block, 0:features]
        scale = jnp.dot(
            rows[block, features : features + LANES],
            select[...],
            preferred_element_type=jnp.float32,
        )
        gate = contract_rows(inputs, weights[0])
        up = contract_rows(inputs, weights[1])
        position = lax.broadcasted_iota(jnp.int32, gate.shape, 1)
        scale = jnp.where(position < hidden, scale, 1.0)
        units = (gate / (1.0 + jnp.exp(-gate)) * up * scale).astype(jnp.bfloat16)
        for c in range(4):
            span = pl.ds(c * width, width)
            parts[k, :, span] = jnp.dot(
                units, weights[2, :, span], preferred_element_type=jnp.float32
            ).astype(jnp.bfloat16)
        part_send(k).start()

        @pl.when(lax.rem(k, 2) == 1)
        def _():
            add_pair(k - 1)
            side_send(j).start()

        @pl.when((k > 0) & (k < depth))
        def _():
            take_weights(nearby(2 * k))

    take_weights(nearby(1))
    for j in range(depth - 1):
        take_weights(nearby(2 * j + 3))
        add_both(j)
        sum_send(j).start()

    for k in range(n):
        source = nearby(k)
        remote(
            slab(source, far_half),
            slab(source, far_half),
            column_out_sem.at[source],
            column_sem.at[source],
            across,
        ).wait_recv()

    add_both(depth - 1)
    for j in range(depth - 1):
        remote(sums.at[0], sums_in.at[j], sum_sem.at[j], sum_recv_sem.at[j], twin).wait_recv()

    @pl.loop(0, row_count // chunk)
    def _(i):
        at = pl.ds(pl.multiple_of(i * chunk, chunk), chunk)
        total = sums[n - 1, at, :].astype(jnp.float32)
        for j in range(depth - 1):
            total = total + sums_in[j, at, :].astype(jnp.float32)
        combined_ref[at, :] = total.astype(jnp.bfloat16)

    @pl.when(outer < depth - 1)
    def _():
        own_up.wait_send()

    @pl.when(outer > 0)
    def _():
        own_back.wait_send()

    for copy in (
        own_beside,
        own_relay,
        shared_far,
        slice_far,
        slice_cross,
        slice_twin,
        shared_twin,
        twin_piece,
        shared_relay,
    ):
        copy.wait_send()

    def sent(place, step):
        source = place * 2 + inner

        @pl.when(onward_exists(step))
        def _():
            row_onward(source, step).wait_send()

        row_beside(source).wait_send()

    for distance in range(1, depth):
        at_distance(distance, sent)
    column_send(fs).wait_send()
    for k in range(1, n):
        d = lax.rem(fs + k, n)
        piece_send(d, 0).wait_send()
        piece_send(d, 1).wait_send()
        column_send(d).wait_send()
        row_relay(d).wait_send()
    for k in range(n):
        part_send(k).wait_send()
    for j in range(depth):
        side_send(j).wait_send()
    for j in range(depth - 1):
        sum_send(j).wait_send()


def direct_body(
    tokens,
    routes,
    route_weights,
    norm_gain,
    gate_trained,
    up_trained,
    down_trained,
    shared_gate_trained,
    shared_up_trained,
    shared_down_trained,
):
    n = lax.axis_size("fs")
    experts, hidden_piece, width = gate_trained.shape
    row_count, features = tokens.shape
    shared_piece = shared_gate_trained.shape[0]
    stacked = (experts * hidden_piece, width)
    hidden = n * hidden_piece
    hidden_all = hidden + shared_piece // 2
    vmem = pl.BlockSpec(memory_space=pltpu.VMEM)
    hbm = pl.BlockSpec(memory_space=pltpu.HBM)
    kind = jnp.bfloat16
    DMA = pltpu.SemaphoreType.DMA
    combined, owned, shared = pl.pallas_call(
        functools.partial(exchange_kernel, n),
        out_shape=(
            jax.ShapeDtypeStruct((row_count, features), kind),
            jax.ShapeDtypeStruct((3, hidden, features), kind),
            jax.ShapeDtypeStruct((3, shared_piece, features), kind),
        ),
        in_specs=[hbm] * 10,
        out_specs=(vmem,) * 3,
        scratch_shapes=[
            pltpu.VMEM((3, hidden_all, features), kind),
            pltpu.VMEM((experts * row_count, features + LANES), kind),
            pltpu.VMEM((LANES, hidden_all), kind),
            pltpu.VMEM((row_count, features), kind),
            pltpu.VMEM(routes.shape[::-1], jnp.int32),
            pltpu.VMEM(routes.shape[::-1], jnp.float32),
            pltpu.VMEM((1, width), jnp.float32),
            pltpu.VMEM((3, shared_piece, width), jnp.float32),
            pltpu.VMEM((3,) + stacked, jnp.float32),
            pltpu.VMEM((3,) + stacked, kind),
            pltpu.VMEM((3, shared_piece, width), kind),
            pltpu.VMEM((n, 2 * row_count, features), kind),
            pltpu.VMEM((n, row_count, features), kind),
            pltpu.VMEM((n, row_count, features), kind),
            pltpu.VMEM((n // 2, row_count, features), kind),
            pltpu.VMEM((n // 2 - 1, row_count, features), kind),
            DMA((5,)),
            DMA((3,)),
            DMA((3,)),
            DMA((n, 2)),
            DMA((n, 2)),
            DMA((n,)),
            DMA((n,)),
            DMA((3,)),
            DMA((3,)),
            DMA((n,)),
            DMA((n // 2,)),
            DMA((1,)),
            DMA((n,)),
            DMA((n,)),
            DMA((n,)),
            DMA((n,)),
            DMA((n,)),
            DMA((n // 2,)),
            DMA((n // 2,)),
            DMA((n // 2 - 1,)),
            DMA((n // 2 - 1,)),
            DMA((3, 2)),
            DMA((7,)),
        ],
        compiler_params=pltpu.CompilerParams(
            collective_id=0, has_side_effects=True, vmem_limit_bytes=48 * 1024 * 1024
        ),
    )(*[
        pltpu.with_memory_space_constraint(array, pltpu.HBM)
        for array in (
            tokens,
            routes.T,
            route_weights.T,
            norm_gain[None, :],
            gate_trained.reshape(stacked),
            up_trained.reshape(stacked),
            down_trained.reshape(stacked),
            shared_gate_trained,
            shared_up_trained,
            shared_down_trained,
        )
    ])
    return settle(combined, owned, shared)


def settle_kernel(combined_ref, owned_ref, shared_ref, combined_out, *refs):
    sems = refs[-1]
    copies = [pltpu.make_async_copy(combined_ref, combined_out, sems.at[6])]
    for j in range(3):
        copies.append(pltpu.make_async_copy(owned_ref.at[j], refs[j].at[0], sems.at[j]))
        copies.append(pltpu.make_async_copy(shared_ref.at[j], refs[3 + j], sems.at[3 + j]))
    for copy in copies:
        copy.start()
    for copy in copies:
        copy.wait()


def settle(combined, owned, shared):
    expert_shape = jax.ShapeDtypeStruct((1,) + owned.shape[1:], owned.dtype)
    shared_shape = jax.ShapeDtypeStruct(shared.shape[1:], shared.dtype)
    return pl.pallas_call(
        settle_kernel,
        out_shape=(jax.ShapeDtypeStruct(combined.shape, combined.dtype),)
        + (expert_shape,) * 3
        + (shared_shape,) * 3,
        in_specs=[pl.BlockSpec(memory_space=pltpu.VMEM)] * 3,
        out_specs=(pl.BlockSpec(memory_space=pltpu.HBM),) * 7,
        scratch_shapes=[pltpu.SemaphoreType.DMA((7,))],
        compiler_params=pltpu.CompilerParams(vmem_limit_bytes=8 * 1024 * 1024),
    )(combined, owned, shared)


def body(*arguments):
    experts = lax.axis_size("fs") * lax.axis_size("tp")
    per_token = arguments[1].shape[1]
    pairs = lax.axis_size("gr") == 2 and lax.axis_size("tp") == 2
    if pairs and lax.axis_size("fs") % 2 == 0 and experts <= min(2 * per_token, LANES // 2):
        return direct_body(*arguments)
    return dispatch_body(*arguments)


def solution(mesh):
    in_specs = (
        P(("gr", "fs", "tp"), None),
        P(("gr", "fs", "tp"), None),
        P(("gr", "fs", "tp"), None),
        P(("gr", "tp")),
        P(None, "fs", ("gr", "tp")),
        P(None, "fs", ("gr", "tp")),
        P(None, "fs", ("gr", "tp")),
        P("fs", ("gr", "tp")),
        P("fs", ("gr", "tp")),
        P("fs", ("gr", "tp")),
    )
    out_specs = (
        P(("gr", "fs", "tp"), None),
        P(("fs", "tp"), None, None),
        P(("fs", "tp"), None, None),
        P(("fs", "tp"), None, None),
        P("fs", None),
        P("fs", None),
        P("fs", None),
    )
    return jax.shard_map(body, mesh=mesh, in_specs=in_specs, out_specs=out_specs, check_vma=False)
```

```python
import functools

import jax
import jax.numpy as jnp
from jax import lax
from jax.experimental import pallas as pl
from jax.experimental.pallas import tpu as pltpu
from jax.sharding import PartitionSpec as P

epsilon = 1e-06
LANES = 128
MESH = pl.DeviceIdType.MESH


def contract_rows(inputs, matrix):
    return lax.dot_general(
        inputs, matrix, (((1,), (1,)), ((), ())), preferred_element_type=jnp.float32
    )


def swiglu_rows(inputs, gate_matrix, up_matrix, down_matrix):
    hidden = (
        jax.nn.silu(contract_rows(inputs, gate_matrix)) * contract_rows(inputs, up_matrix)
    ).astype(jnp.bfloat16)
    return jnp.dot(hidden, down_matrix, preferred_element_type=jnp.float32)


def dispatch_body(
    tokens,
    routes,
    route_weights,
    norm_gain,
    gate_trained,
    up_trained,
    down_trained,
    shared_gate_trained,
    shared_up_trained,
    shared_down_trained,
):
    gain_row = norm_gain[None, None, :]
    stacked = jnp.stack(
        [gate_trained * gain_row, up_trained * gain_row, down_trained], axis=1
    ).astype(jnp.bfloat16)
    halves = lax.all_to_all(
        lax.all_to_all(stacked[:, :, :, None, :], "fs", split_axis=0, concat_axis=2, tiled=True),
        "tp",
        split_axis=0,
        concat_axis=3,
        tiled=True,
    )
    owned = lax.all_gather(halves[:, :, :, None], "gr", axis=3, tiled=True)
    owned = owned.reshape(owned.shape[0], 3, owned.shape[2], -1)
    expert_gate = owned[:, 0]
    expert_up = owned[:, 1]
    expert_down = owned[:, 2]
    shared_gain = norm_gain[None, :]
    shared_stack = jnp.stack(
        [shared_gate_trained * shared_gain, shared_up_trained * shared_gain, shared_down_trained],
        axis=0,
    ).astype(jnp.bfloat16)
    shared_whole = lax.all_gather(shared_stack, ("gr", "tp"), axis=2, tiled=True)
    shared_gate = shared_whole[0]
    shared_up = shared_whole[1]
    shared_down = shared_whole[2]
    values = tokens.astype(jnp.float32)
    normed = (
        values * lax.rsqrt(jnp.mean(values * values, axis=1, keepdims=True) + epsilon)
    ).astype(jnp.bfloat16)
    row_count, features = normed.shape
    per_token = routes.shape[1]
    shared_out = swiglu_rows(
        normed,
        lax.all_gather(shared_gate, "fs", axis=0, tiled=True),
        lax.all_gather(shared_up, "fs", axis=0, tiled=True),
        lax.all_gather(shared_down, "fs", axis=0, tiled=True),
    )
    experts = lax.axis_size("fs") * lax.axis_size("tp")
    capacity = max(2, 3 * row_count * per_token // (2 * experts))
    chosen = routes.reshape(-1)
    onehot = (chosen[:, None] == jnp.arange(experts, dtype=jnp.int32)[None, :]).astype(jnp.int32)
    position = jnp.sum((jnp.cumsum(onehot, axis=0) - onehot) * onehot, axis=1)
    target = chosen * capacity + position
    source = (
        jnp.full((experts * capacity,), row_count, jnp.int32)
        .at[target]
        .set(jnp.arange(row_count * per_token, dtype=jnp.int32) // per_token)
    )
    padded = jnp.concatenate([normed, jnp.zeros((1, features), jnp.bfloat16)], axis=0)
    outgoing = padded[source].reshape(experts, capacity, features)
    arrived = lax.all_to_all(outgoing, ("fs", "tp"), split_axis=0, concat_axis=0, tiled=True)
    item_count = arrived.shape[1]
    result = swiglu_rows(
        arrived.reshape(-1, features), expert_gate[0], expert_up[0], expert_down[0]
    )
    result = result.astype(jnp.bfloat16).reshape(experts, item_count, features)
    returned = lax.all_to_all(result, ("fs", "tp"), split_axis=0, concat_axis=0, tiled=True)
    picked = returned.reshape(experts * capacity, features)[target].astype(jnp.float32)
    picked = picked.reshape(row_count, per_token, features)
    routed = jnp.sum(picked * route_weights[:, :, None], axis=1)
    combined = (routed + shared_out).astype(jnp.bfloat16)
    return (combined, expert_gate, expert_up, expert_down, shared_gate, shared_up, shared_down)


def exchange_kernel(
    n,
    tokens_hbm,
    routes_hbm,
    route_weights_hbm,
    gain_hbm,
    gate_hbm,
    up_hbm,
    down_hbm,
    shared_gate_hbm,
    shared_up_hbm,
    shared_down_hbm,
    combined_ref,
    owned,
    shared,
    weights,
    rows,
    select,
    tokens_ref,
    routes_ref,
    route_weights_ref,
    gain_ref,
    shared_stage,
    stage,
    pieces,
    guests,
    shared_mine,
    parts,
    pair_in,
    sums,
    side_in,
    mate_in,
    sums_in,
    local_sem,
    slice_out_sem,
    slice_sem,
    piece_sem,
    guest_out_sem,
    guest_sem,
    guest_on_sem,
    weight_sem,
    column_out_sem,
    column_sem,
    shared_out_sem,
    shared_sem,
    row_out_sem,
    row_side_sem,
    row_back_sem,
    row_sem,
    mix_out_sem,
    mix_back_sem,
    mix_sem,
    row_pair_out_sem,
    row_pair_sem,
    part_sem,
    part_recv_sem,
    side_sem,
    side_recv_sem,
    sum_sem,
    mate_sem,
    sum_recv_sem,
    stage_sem,
    input_sem,
):
    gr, fs, tp = lax.axis_index("gr"), lax.axis_index("fs"), lax.axis_index("tp")
    other = 1 - tp
    across = (1 - gr, fs, tp)
    across_twin = (1 - gr, fs, other)
    twin = (gr, fs, other)
    expert = fs * 2 + tp
    width = pieces.shape[2]
    hidden_piece = pieces.shape[1] // (2 * n)
    hidden = n * hidden_piece
    shared_piece = shared_mine.shape[1]
    extra = shared_piece // 2
    features = 4 * width
    row_count = tokens_ref.shape[0]
    depth = n // 2
    outer, inner = lax.div(fs, 2), lax.rem(fs, 2)
    beside = (gr, outer * 2 + 1 - inner, tp)
    toward = jnp.where(outer < depth // 2, 1, -1)

    inputs_in = []
    for i, (source, target) in enumerate(
        (
            (tokens_hbm, tokens_ref),
            (routes_hbm, routes_ref),
            (route_weights_hbm, route_weights_ref),
            (gain_hbm, gain_ref),
            (shared_gate_hbm, shared_stage.at[0]),
            (shared_up_hbm, shared_stage.at[1]),
            (shared_down_hbm, shared_stage.at[2]),
        )
    ):
        inputs_in.append(pltpu.make_async_copy(source, target, input_sem.at[i]))
        inputs_in[i].start()
    staged = {}
    for t in (0, 1):
        for j, ref in enumerate((gate_hbm, up_hbm, down_hbm)):
            part = pl.ds(t * hidden, hidden)
            staged[j, t] = pltpu.make_async_copy(ref.at[part], stage.at[j, part], stage_sem.at[j, t])
            staged[j, t].start()

    barrier = pltpu.get_barrier_semaphore()
    for device in (across, across_twin, twin):
        pl.semaphore_signal(barrier, inc=1, device_id=device, device_id_type=MESH)
    for k in range(1, n):
        for t in range(2):
            pl.semaphore_signal(
                barrier, inc=1, device_id=(gr, lax.rem(fs + k, n), t), device_id_type=MESH
            )

    own_start = pl.multiple_of(expert * row_count, row_count)
    few = 16
    for copy in inputs_in:
        copy.wait()

    @pl.loop(0, row_count // few)
    def _(i):
        at = pl.multiple_of(i * few, few)
        values = tokens_ref[pl.ds(at, few), :].astype(jnp.float32)
        mean = jnp.mean(values * values, axis=1, keepdims=True)
        normed = (values * lax.rsqrt(mean + epsilon)).astype(jnp.bfloat16)
        rows[pl.ds(own_start + at, few), 0:features] = normed

    number = lax.broadcasted_iota(jnp.int32, (LANES // 2, row_count), 0)
    factors = jnp.zeros(number.shape, jnp.float32)
    for k in range(routes_ref.shape[0]):
        named = routes_ref[k : k + 1, :] == number
        factors = factors + jnp.where(named, route_weights_ref[k : k + 1, :], 0.0)
    high = factors.astype(jnp.bfloat16).astype(jnp.float32)
    both = jnp.concatenate([high, factors - high], axis=0)
    rows[pl.ds(own_start, row_count), features : features + LANES] = both.T.astype(jnp.bfloat16)

    gain = gain_ref[...]
    for j in range(3):
        value = shared_stage[j] if j == 2 else shared_stage[j] * gain
        shared_mine[j] = value.astype(jnp.bfloat16)
    for t in (0, 1):
        for j in range(3):
            staged[j, t].wait()

            @pl.loop(0, n)
            def _(i):
                at = pl.ds(pl.multiple_of((t * n + i) * hidden_piece, hidden_piece), hidden_piece)
                value = stage[j, at, :] if j == 2 else stage[j, at, :] * gain_ref[...]
                pieces[j, at, :] = value.astype(jnp.bfloat16)

    lane = lax.broadcasted_iota(jnp.int32, select.shape, 0)
    unit = lax.broadcasted_iota(jnp.int32, select.shape, 1)
    first = (jnp.where(lane < LANES // 2, lane, lane - LANES // 2) - tp * n) * hidden_piece
    inside = (unit >= first) & (unit < first + hidden_piece) & (unit < hidden)
    select[...] = jnp.where(inside, 1.0, 0.0).astype(select.dtype)
    pl.semaphore_wait(barrier, 2 * n + 1)

    def remote(src, dst, send, recv, device):
        return pltpu.make_async_remote_copy(
            src_ref=src,
            dst_ref=dst,
            send_sem=send,
            recv_sem=recv,
            device_id=device,
            device_id_type=MESH,
        )

    def columns(g, t):
        return pl.ds(pl.multiple_of((g * 2 + t) * width, width), width)

    def piece(e):
        return pieces.at[:, pl.ds(pl.multiple_of(e * hidden_piece, 16), hidden_piece), :]

    def portion(t):
        return pieces.at[:, pl.ds(pl.multiple_of(t * hidden, 16), hidden), :]

    def sliced(g, t):
        return weights.at[:, pl.ds(0, hidden), columns(g, t)]

    def slab(source, span):
        start = pl.multiple_of(source * hidden_piece, 16)
        return owned.at[:, pl.ds(start, hidden_piece), span]

    def row_block(source, t):
        start = pl.multiple_of((source * 2 + t) * row_count, row_count)
        return rows.at[pl.ds(start, row_count)]

    late = row_count // 4
    early = row_count - late

    def row_early(source):
        start = pl.multiple_of((source * 2 + tp) * row_count, row_count)
        return rows.at[pl.ds(start, early)]

    def row_late(source):
        start = pl.multiple_of((source * 2 + tp) * row_count, row_count)
        return rows.at[pl.ds(pl.multiple_of(start + early, late), late)]

    def nearby(k):
        place = lax.rem(outer + toward * lax.div(k, 2) + depth, depth)
        return place * 2 + jnp.where(lax.rem(k, 2) == 0, inner, 1 - inner)

    half = pl.ds(pl.multiple_of(gr * 2 * width, width), 2 * width)
    far_half = pl.ds(pl.multiple_of((1 - gr) * 2 * width, width), 2 * width)

    def slice_send(index, t, device):
        return remote(
            portion(t), sliced(gr, tp), slice_out_sem.at[index], slice_sem.at[index], device
        )

    def piece_send(d, t):
        return remote(
            piece(d * 2 + t),
            slab(fs, columns(gr, tp)),
            piece_sem.at[d, t],
            weight_sem.at[fs, tp],
            (gr, d, t),
        )

    pair = 2 * hidden_piece

    def guest_send(place):
        start = pl.multiple_of((place * 2 + 1 - inner) * pair, 16)
        spot = pl.ds(place * pair, pair)
        return remote(
            pieces.at[:, pl.ds(start, pair), :],
            guests.at[:, spot, :],
            guest_out_sem.at[place],
            guest_sem.at[place],
            beside,
        )

    fs_beside = outer * 2 + 1 - inner

    def guest(place, t):
        start = pl.multiple_of(place * pair + t * hidden_piece, 16)
        return guests.at[:, pl.ds(start, hidden_piece), :]

    def guest_onward(place, t):
        return remote(
            guest(place, t),
            slab(fs_beside, columns(gr, tp)),
            guest_on_sem.at[place, t],
            weight_sem.at[fs_beside, tp],
            (gr, place * 2 + inner, t),
        )

    guest_local = pltpu.make_async_copy(
        guest(outer, tp), slab(fs_beside, columns(gr, tp)), local_sem.at[0]
    )

    def column_send(source):
        return remote(
            slab(source, half),
            slab(source, half),
            column_out_sem.at[source],
            column_sem.at[source],
            across,
        )

    def row_move(source, send, recv, device):
        return remote(row_block(source, tp), row_block(source, tp), send, recv, device)

    def row_onward(source, step):
        return row_move(
            source,
            row_out_sem.at[source],
            row_sem.at[source],
            (gr, (outer + step) * 2 + inner, tp),
        )

    def row_beside(source, distance):
        block = row_early(source) if distance < depth - 1 else row_block(source, tp)
        return remote(block, block, row_side_sem.at[lax.div(source, 2)], row_sem.at[source], beside)

    def mixed(place, send, step):
        block = row_late(place * 2 + 1 - inner)
        device = (gr, (outer + step) * 2 + inner, tp)
        return remote(block, block, send, mix_sem.at[place], device)

    mix_up = mixed(outer, mix_out_sem.at[outer], 1)
    mix_back = mixed(outer, mix_back_sem.at[0], -1)

    def row_relay(source):
        return row_move(source, row_pair_out_sem.at[source], row_pair_sem.at[source], twin)

    own_up = row_move(fs, row_out_sem.at[fs], row_sem.at[fs], (gr, (outer + 1) * 2 + inner, tp))
    own_back = row_move(fs, row_back_sem.at[0], row_sem.at[fs], (gr, (outer - 1) * 2 + inner, tp))
    own_beside = row_move(fs, row_side_sem.at[outer], row_sem.at[fs], beside)
    own_relay = row_move(fs, row_pair_out_sem.at[fs], row_pair_sem.at[fs], twin)

    def at_distance(distance, action):
        for step in (-1, 1):
            place = outer - step * distance

            @pl.when((place >= 0) & (place < depth))
            def _():
                action(place, step, distance)

    def onward_exists(step):
        return (outer + step >= 0) & (outer + step < depth)

    @pl.when(outer < depth - 1)
    def _():
        own_up.start()

    @pl.when(outer > 0)
    def _():
        own_back.start()

    own_beside.start()
    shared_far = remote(
        shared_mine, shared.at[:, :, columns(gr, tp)], shared_out_sem.at[0], shared_sem.at[0], across
    )
    shared_far.start()
    slice_far = slice_send(0, tp, across)
    slice_cross = slice_send(1, other, across_twin)
    slice_twin = slice_send(2, other, twin)
    slice_far.start()
    slice_cross.start()
    own_relay.start()
    slice_twin.start()
    shared_twin = remote(
        shared_mine, shared.at[:, :, columns(gr, tp)], shared_out_sem.at[1], shared_sem.at[1], twin
    )
    shared_twin.start()
    twin_piece = piece_send(fs, other)
    twin_piece.start()

    def ship(places):
        for place in places:

            @pl.when(place != outer)
            def _():
                piece_send(place * 2 + inner, 0).start()
                piece_send(place * 2 + inner, 1).start()

    own_slice = pltpu.make_async_copy(portion(tp), sliced(gr, tp), local_sem.at[1])
    own_piece = pltpu.make_async_copy(piece(expert), slab(fs, columns(gr, tp)), local_sem.at[2])
    own_shared = pltpu.make_async_copy(
        shared_mine, shared.at[:, :, columns(gr, tp)], local_sem.at[3]
    )
    locals_ = (own_slice, own_piece, own_shared)
    for copy in locals_:
        copy.start()

    def take_rows(source):
        row_move(source, row_out_sem.at[source], row_sem.at[source], twin).wait_recv()

    def arrive(place, step, distance):
        source = place * 2 + inner
        take_rows(source)

        @pl.when(onward_exists(step))
        def _():
            row_onward(source, step).start()

        row_beside(source, distance).start()
        row_relay(source).start()

    def arrive_mixed(place, step, distance):
        mixed(place, mix_out_sem.at[place], step).wait_recv()
        if distance < depth - 2:

            @pl.when(onward_exists(step))
            def _():
                mixed(place, mix_out_sem.at[place], step).start()

    def arrive_beside(place, step, distance):
        source = place * 2 + 1 - inner
        row_beside(source, distance).wait_recv()
        row_relay(source).start()

    at_distance(1, arrive)
    take_rows(outer * 2 + 1 - inner)

    @pl.when(outer < depth - 1)
    def _():
        mix_up.start()

    @pl.when(outer > 0)
    def _():
        mix_back.start()

    row_relay(outer * 2 + 1 - inner).start()
    for place in range(depth):
        guest_send(place).start()
    for copy in locals_:
        copy.wait()
    far_columns = shared.at[:, :, columns(1 - gr, tp)]
    remote(shared_mine, far_columns, shared_out_sem.at[0], shared_sem.at[0], across).wait_recv()
    shared_relay = remote(far_columns, far_columns, shared_out_sem.at[2], shared_sem.at[2], twin)
    shared_relay.start()
    at_distance(2, arrive)
    ship(range(1, depth - 1))
    at_distance(1, arrive_mixed)
    at_distance(1, arrive_beside)
    at_distance(3, arrive)
    at_distance(2, arrive_mixed)
    ship((0, depth - 1))

    for place in range(depth):
        guest_send(place).wait_recv()

        @pl.when(place != outer)
        def _():
            guest_onward(place, 0).start()
            guest_onward(place, 1).start()

    guest_onward(outer, other).start()
    guest_local.start()
    guest_local.wait()

    def take_twin_piece(source, t):
        remote(
            piece(0),
            slab(source, columns(gr, t)),
            piece_sem.at[fs, other],
            weight_sem.at[source, t],
            twin,
        ).wait_recv()

    take_twin_piece(fs, other)
    column_send(fs).start()

    remote(
        shared_mine, shared.at[:, :, columns(gr, other)], shared_out_sem.at[1], shared_sem.at[1], twin
    ).wait_recv()
    last_columns = shared.at[:, :, columns(1 - gr, other)]
    remote(shared_mine, last_columns, shared_out_sem.at[2], shared_sem.at[2], twin).wait_recv()
    tail = pltpu.make_async_copy(
        shared.at[:, pl.ds(pl.multiple_of(tp * extra, extra), extra), :],
        weights.at[:, pl.ds(hidden, extra), :],
        local_sem.at[4],
    )
    tail.start()
    tail.wait()
    remote(portion(tp), sliced(gr, other), slice_out_sem.at[2], slice_sem.at[2], twin).wait_recv()
    remote(portion(tp), sliced(1 - gr, tp), slice_out_sem.at[0], slice_sem.at[0], across).wait_recv()
    remote(
        portion(tp), sliced(1 - gr, other), slice_out_sem.at[1], slice_sem.at[1], across
    ).wait_recv()

    def part_send(k):
        return remote(
            parts.at[k, pl.ds(pl.multiple_of(other * row_count, row_count), row_count), :],
            pair_in.at[k],
            part_sem.at[k],
            part_recv_sem.at[k],
            twin,
        )

    low = outer < depth // 2
    near = jnp.where(low, 1, 2 * depth - 3) - outer
    at_end = (outer == 0) | (outer == depth - 1)

    def place_of(j):
        far = jnp.where(low, depth // 2 + j, depth // 2 - 1 - j)
        return jnp.where(j < depth // 2, far, jnp.where(j == depth - 1, outer, near))

    def side_send(j):
        return remote(
            sums.at[2 * j], side_in.at[j], side_sem.at[j], side_recv_sem.at[j], beside
        )

    def mate_send(j):
        return remote(
            sums.at[2 * j + 1],
            mate_in.at[j],
            sum_sem.at[j],
            mate_sem.at[j],
            (gr, near * 2 + inner, tp),
        )

    def sum_send(j):
        slot = 1 if j < depth // 2 else 0
        return remote(
            sums.at[2 * j + 1],
            sums_in.at[slot],
            sum_sem.at[j],
            sum_recv_sem.at[slot],
            (gr, place_of(j) * 2 + inner, tp),
        )

    chunk = 32

    def add_pair(k):
        part_send(k).wait_recv()

        @pl.loop(0, row_count // chunk)
        def _(i):
            at = pl.multiple_of(i * chunk, chunk)
            mine = pl.multiple_of(tp * row_count + i * chunk, chunk)
            value = parts[k, pl.ds(mine, chunk), :].astype(jnp.float32)
            value = value + pair_in[k, pl.ds(at, chunk), :].astype(jnp.float32)
            sums[k, pl.ds(at, chunk), :] = value.astype(jnp.bfloat16)

    def await_both(j):
        part_send(2 * j + 1).wait_recv()
        side_send(j).wait_recv()

    def add_both(j, mate):
        k = 2 * j + 1

        @pl.loop(0, row_count // chunk)
        def _(i):
            at = pl.multiple_of(i * chunk, chunk)
            mine = pl.multiple_of(tp * row_count + i * chunk, chunk)
            value = parts[k, pl.ds(mine, chunk), :].astype(jnp.float32)
            value = value + pair_in[k, pl.ds(at, chunk), :].astype(jnp.float32)
            value = value + side_in[j, pl.ds(at, chunk), :].astype(jnp.float32)
            if mate:
                value = value + mate_in[j, pl.ds(at, chunk), :].astype(jnp.float32)
            sums[k, pl.ds(at, chunk), :] = value.astype(jnp.bfloat16)

    def take_weights(source):
        take_twin_piece(source, 0)
        take_twin_piece(source, 1)
        column_send(source).start()

    def pass_far(j):
        await_both(j)

        @pl.when(at_end)
        def _():
            add_both(j, False)
            mate_send(j).start()

        @pl.when(jnp.logical_not(at_end))
        def _():
            mate_send(j).wait_recv()
            add_both(j, True)
            sum_send(j).start()

    def pass_near(j):
        await_both(j)
        add_both(j, False)
        sum_send(j).start()

    @pl.loop(0, n)
    def _(k):
        j = lax.div(k, 2)
        d = place_of(j) * 2 + jnp.where(lax.rem(k, 2) == 0, 1 - inner, inner)

        @pl.when(k == jnp.where(at_end, 0, 2))
        def _():
            at_distance(2, arrive_beside)

        @pl.when(k == 2)
        def _():
            at_distance(3, arrive_beside)

        remote(
            row_block(d, other), row_block(d, other), row_pair_out_sem.at[d], row_pair_sem.at[d], twin
        ).wait_recv()
        block = pl.ds(pl.multiple_of(d * 2 * row_count, 2 * row_count), 2 * row_count)
        inputs = rows[block, 0:features]
        scale = jnp.dot(
            rows[block, features : features + LANES],
            select[...],
            preferred_element_type=jnp.float32,
        )
        gate = contract_rows(inputs, weights[0])
        up = contract_rows(inputs, weights[1])
        position = lax.broadcasted_iota(jnp.int32, gate.shape, 1)
        scale = jnp.where(position < hidden, scale, 1.0)
        units = (gate / (1.0 + jnp.exp(-gate)) * up * scale).astype(jnp.bfloat16)
        for c in range(4):
            span = pl.ds(c * width, width)
            parts[k, :, span] = jnp.dot(
                units, weights[2, :, span], preferred_element_type=jnp.float32
            ).astype(jnp.bfloat16)
        part_send(k).start()

        @pl.when(lax.rem(k, 2) == 1)
        def _():
            add_pair(k - 1)
            side_send(j).start()

        @pl.when((k > 0) & (k < depth))
        def _():
            take_weights(nearby(2 * k))

        @pl.when((k == n - 3) & at_end)
        def _():
            pass_far(0)

    take_twin_piece(fs_beside, other)
    column_send(fs_beside).start()

    @pl.when(jnp.logical_not(at_end))
    def _():
        pass_far(0)
        pass_near(2)

    take_weights(nearby(3))
    pass_far(1)
    take_weights(nearby(5))

    @pl.when(at_end)
    def _():
        pass_near(2)

    take_weights(nearby(7))

    for k in range(n):
        source = nearby(k)
        remote(
            slab(source, far_half),
            slab(source, far_half),
            column_out_sem.at[source],
            column_sem.at[source],
            across,
        ).wait_recv()

    await_both(depth - 1)
    add_both(depth - 1, False)
    for j in range(2):
        remote(sums.at[0], sums_in.at[j], sum_sem.at[j], sum_recv_sem.at[j], twin).wait_recv()

    @pl.loop(0, row_count // chunk)
    def _(i):
        at = pl.ds(pl.multiple_of(i * chunk, chunk), chunk)
        total = sums[n - 1, at, :].astype(jnp.float32)
        for j in range(2):
            total = total + sums_in[j, at, :].astype(jnp.float32)
        combined_ref[at, :] = total.astype(jnp.bfloat16)

    @pl.when(outer < depth - 1)
    def _():
        own_up.wait_send()
        mix_up.wait_send()

    @pl.when(outer > 0)
    def _():
        own_back.wait_send()
        mix_back.wait_send()

    for copy in (
        own_beside,
        own_relay,
        shared_far,
        slice_far,
        slice_cross,
        slice_twin,
        shared_twin,
        twin_piece,
        shared_relay,
    ):
        copy.wait_send()

    def sent(place, step, distance):
        source = place * 2 + inner

        @pl.when(onward_exists(step))
        def _():
            row_onward(source, step).wait_send()
            if distance < depth - 2:
                mixed(place, mix_out_sem.at[place], step).wait_send()

        row_beside(source, distance).wait_send()

    for distance in range(1, depth):
        at_distance(distance, sent)
    column_send(fs).wait_send()
    for k in range(1, n):
        d = lax.rem(fs + k, n)
        column_send(d).wait_send()
        row_relay(d).wait_send()
    for place in range(depth):
        guest_send(place).wait_send()

        @pl.when(place != outer)
        def _():
            for t in range(2):
                piece_send(place * 2 + inner, t).wait_send()
                guest_onward(place, t).wait_send()

    guest_onward(outer, other).wait_send()
    for k in range(n):
        part_send(k).wait_send()
    for j in range(depth):
        side_send(j).wait_send()
    for j in range(depth - 1):
        sum_send(j).wait_send()


def direct_body(
    tokens,
    routes,
    route_weights,
    norm_gain,
    gate_trained,
    up_trained,
    down_trained,
    shared_gate_trained,
    shared_up_trained,
    shared_down_trained,
):
    n = lax.axis_size("fs")
    experts, hidden_piece, width = gate_trained.shape
    row_count, features = tokens.shape
    shared_piece = shared_gate_trained.shape[0]
    stacked = (experts * hidden_piece, width)
    hidden = n * hidden_piece
    hidden_all = hidden + shared_piece // 2
    vmem = pl.BlockSpec(memory_space=pltpu.VMEM)
    hbm = pl.BlockSpec(memory_space=pltpu.HBM)
    kind = jnp.bfloat16
    DMA = pltpu.SemaphoreType.DMA
    combined, owned, shared = pl.pallas_call(
        functools.partial(exchange_kernel, n),
        out_shape=(
            jax.ShapeDtypeStruct((row_count, features), kind),
            jax.ShapeDtypeStruct((3, hidden, features), kind),
            jax.ShapeDtypeStruct((3, shared_piece, features), kind),
        ),
        in_specs=[hbm] * 10,
        out_specs=(vmem,) * 3,
        scratch_shapes=[
            pltpu.VMEM((3, hidden_all, features), kind),
            pltpu.VMEM((experts * row_count, features + LANES), kind),
            pltpu.VMEM((LANES, hidden_all), kind),
            pltpu.VMEM((row_count, features), kind),
            pltpu.VMEM(routes.shape[::-1], jnp.int32),
            pltpu.VMEM(routes.shape[::-1], jnp.float32),
            pltpu.VMEM((1, width), jnp.float32),
            pltpu.VMEM((3, shared_piece, width), jnp.float32),
            pltpu.VMEM((3,) + stacked, jnp.float32),
            pltpu.VMEM((3,) + stacked, kind),
            pltpu.VMEM((3, n * hidden_piece, width), kind),
            pltpu.VMEM((3, shared_piece, width), kind),
            pltpu.VMEM((n, 2 * row_count, features), kind),
            pltpu.VMEM((n, row_count, features), kind),
            pltpu.VMEM((n, row_count, features), kind),
            pltpu.VMEM((n // 2, row_count, features), kind),
            pltpu.VMEM((n // 4, row_count, features), kind),
            pltpu.VMEM((2, row_count, features), kind),
            DMA((5,)),
            DMA((3,)),
            DMA((3,)),
            DMA((n, 2)),
            DMA((n // 2,)),
            DMA((n // 2,)),
            DMA((n // 2, 2)),
            DMA((n, 2)),
            DMA((n,)),
            DMA((n,)),
            DMA((3,)),
            DMA((3,)),
            DMA((n,)),
            DMA((n // 2,)),
            DMA((1,)),
            DMA((n,)),
            DMA((n // 2,)),
            DMA((1,)),
            DMA((n // 2,)),
            DMA((n,)),
            DMA((n,)),
            DMA((n,)),
            DMA((n,)),
            DMA((n // 2,)),
            DMA((n // 2,)),
            DMA((n // 2 - 1,)),
            DMA((n // 4,)),
            DMA((2,)),
            DMA((3, 2)),
            DMA((7,)),
        ],
        compiler_params=pltpu.CompilerParams(
            collective_id=0, has_side_effects=True, vmem_limit_bytes=48 * 1024 * 1024
        ),
    )(*[
        pltpu.with_memory_space_constraint(array, pltpu.HBM)
        for array in (
            tokens,
            routes.T,
            route_weights.T,
            norm_gain[None, :],
            gate_trained.reshape(stacked),
            up_trained.reshape(stacked),
            down_trained.reshape(stacked),
            shared_gate_trained,
            shared_up_trained,
            shared_down_trained,
        )
    ])
    return settle(combined, owned, shared)


def settle_kernel(combined_ref, owned_ref, shared_ref, combined_out, *refs):
    sems = refs[-1]
    copies = [pltpu.make_async_copy(combined_ref, combined_out, sems.at[6])]
    for j in range(3):
        copies.append(pltpu.make_async_copy(owned_ref.at[j], refs[j].at[0], sems.at[j]))
        copies.append(pltpu.make_async_copy(shared_ref.at[j], refs[3 + j], sems.at[3 + j]))
    for copy in copies:
        copy.start()
    for copy in copies:
        copy.wait()


def settle(combined, owned, shared):
    expert_shape = jax.ShapeDtypeStruct((1,) + owned.shape[1:], owned.dtype)
    shared_shape = jax.ShapeDtypeStruct(shared.shape[1:], shared.dtype)
    return pl.pallas_call(
        settle_kernel,
        out_shape=(jax.ShapeDtypeStruct(combined.shape, combined.dtype),)
        + (expert_shape,) * 3
        + (shared_shape,) * 3,
        in_specs=[pl.BlockSpec(memory_space=pltpu.VMEM)] * 3,
        out_specs=(pl.BlockSpec(memory_space=pltpu.HBM),) * 7,
        scratch_shapes=[pltpu.SemaphoreType.DMA((7,))],
        compiler_params=pltpu.CompilerParams(vmem_limit_bytes=8 * 1024 * 1024),
    )(combined, owned, shared)


def body(*arguments):
    experts = lax.axis_size("fs") * lax.axis_size("tp")
    per_token = arguments[1].shape[1]
    pairs = lax.axis_size("gr") == 2 and lax.axis_size("tp") == 2
    if pairs and lax.axis_size("fs") == 8 and experts <= min(2 * per_token, LANES // 2):
        return direct_body(*arguments)
    return dispatch_body(*arguments)


def solution(mesh):
    in_specs = (
        P(("gr", "fs", "tp"), None),
        P(("gr", "fs", "tp"), None),
        P(("gr", "fs", "tp"), None),
        P(("gr", "tp")),
        P(None, "fs", ("gr", "tp")),
        P(None, "fs", ("gr", "tp")),
        P(None, "fs", ("gr", "tp")),
        P("fs", ("gr", "tp")),
        P("fs", ("gr", "tp")),
        P("fs", ("gr", "tp")),
    )
    out_specs = (
        P(("gr", "fs", "tp"), None),
        P(("fs", "tp"), None, None),
        P(("fs", "tp"), None, None),
        P(("fs", "tp"), None, None),
        P("fs", None),
        P("fs", None),
        P("fs", None),
    )
    return jax.shard_map(body, mesh=mesh, in_specs=in_specs, out_specs=out_specs, check_vma=False)
```

```python
import functools

import jax
import jax.numpy as jnp
from jax import lax
from jax.experimental import pallas as pl
from jax.experimental.pallas import tpu as pltpu
from jax.sharding import PartitionSpec as P

epsilon = 1e-06
LANES = 128
MESH = pl.DeviceIdType.MESH


def contract_rows(inputs, matrix):
    return lax.dot_general(
        inputs, matrix, (((1,), (1,)), ((), ())), preferred_element_type=jnp.float32
    )


def swiglu_rows(inputs, gate_matrix, up_matrix, down_matrix):
    hidden = (
        jax.nn.silu(contract_rows(inputs, gate_matrix)) * contract_rows(inputs, up_matrix)
    ).astype(jnp.bfloat16)
    return jnp.dot(hidden, down_matrix, preferred_element_type=jnp.float32)


def dispatch_body(
    tokens,
    routes,
    route_weights,
    norm_gain,
    gate_trained,
    up_trained,
    down_trained,
    shared_gate_trained,
    shared_up_trained,
    shared_down_trained,
):
    gain_row = norm_gain[None, None, :]
    stacked = jnp.stack(
        [gate_trained * gain_row, up_trained * gain_row, down_trained], axis=1
    ).astype(jnp.bfloat16)
    halves = lax.all_to_all(
        lax.all_to_all(stacked[:, :, :, None, :], "fs", split_axis=0, concat_axis=2, tiled=True),
        "tp",
        split_axis=0,
        concat_axis=3,
        tiled=True,
    )
    owned = lax.all_gather(halves[:, :, :, None], "gr", axis=3, tiled=True)
    owned = owned.reshape(owned.shape[0], 3, owned.shape[2], -1)
    expert_gate = owned[:, 0]
    expert_up = owned[:, 1]
    expert_down = owned[:, 2]
    shared_gain = norm_gain[None, :]
    shared_stack = jnp.stack(
        [shared_gate_trained * shared_gain, shared_up_trained * shared_gain, shared_down_trained],
        axis=0,
    ).astype(jnp.bfloat16)
    shared_whole = lax.all_gather(shared_stack, ("gr", "tp"), axis=2, tiled=True)
    shared_gate = shared_whole[0]
    shared_up = shared_whole[1]
    shared_down = shared_whole[2]
    values = tokens.astype(jnp.float32)
    normed = (
        values * lax.rsqrt(jnp.mean(values * values, axis=1, keepdims=True) + epsilon)
    ).astype(jnp.bfloat16)
    row_count, features = normed.shape
    per_token = routes.shape[1]
    shared_out = swiglu_rows(
        normed,
        lax.all_gather(shared_gate, "fs", axis=0, tiled=True),
        lax.all_gather(shared_up, "fs", axis=0, tiled=True),
        lax.all_gather(shared_down, "fs", axis=0, tiled=True),
    )
    experts = lax.axis_size("fs") * lax.axis_size("tp")
    capacity = max(2, 3 * row_count * per_token // (2 * experts))
    chosen = routes.reshape(-1)
    onehot = (chosen[:, None] == jnp.arange(experts, dtype=jnp.int32)[None, :]).astype(jnp.int32)
    position = jnp.sum((jnp.cumsum(onehot, axis=0) - onehot) * onehot, axis=1)
    target = chosen * capacity + position
    source = (
        jnp.full((experts * capacity,), row_count, jnp.int32)
        .at[target]
        .set(jnp.arange(row_count * per_token, dtype=jnp.int32) // per_token)
    )
    padded = jnp.concatenate([normed, jnp.zeros((1, features), jnp.bfloat16)], axis=0)
    outgoing = padded[source].reshape(experts, capacity, features)
    arrived = lax.all_to_all(outgoing, ("fs", "tp"), split_axis=0, concat_axis=0, tiled=True)
    item_count = arrived.shape[1]
    result = swiglu_rows(
        arrived.reshape(-1, features), expert_gate[0], expert_up[0], expert_down[0]
    )
    result = result.astype(jnp.bfloat16).reshape(experts, item_count, features)
    returned = lax.all_to_all(result, ("fs", "tp"), split_axis=0, concat_axis=0, tiled=True)
    picked = returned.reshape(experts * capacity, features)[target].astype(jnp.float32)
    picked = picked.reshape(row_count, per_token, features)
    routed = jnp.sum(picked * route_weights[:, :, None], axis=1)
    combined = (routed + shared_out).astype(jnp.bfloat16)
    return (combined, expert_gate, expert_up, expert_down, shared_gate, shared_up, shared_down)


def exchange_kernel(
    n,
    tokens_hbm,
    routes_hbm,
    route_weights_hbm,
    gain_hbm,
    gate_hbm,
    up_hbm,
    down_hbm,
    shared_gate_hbm,
    shared_up_hbm,
    shared_down_hbm,
    combined_ref,
    owned,
    shared,
    weights,
    rows,
    select,
    tokens_ref,
    routes_ref,
    route_weights_ref,
    gain_ref,
    shared_stage,
    stage,
    pieces,
    guests,
    shared_mine,
    parts,
    pair_in,
    sums,
    side_in,
    mate_in,
    sums_in,
    local_sem,
    slice_out_sem,
    slice_sem,
    piece_sem,
    guest_out_sem,
    guest_sem,
    guest_on_sem,
    weight_sem,
    column_out_sem,
    column_sem,
    shared_out_sem,
    shared_sem,
    row_out_sem,
    row_side_sem,
    row_back_sem,
    row_sem,
    mix_out_sem,
    mix_back_sem,
    mix_sem,
    row_pair_out_sem,
    row_pair_sem,
    part_sem,
    part_recv_sem,
    side_sem,
    side_recv_sem,
    sum_sem,
    mate_sem,
    sum_recv_sem,
    stage_sem,
    input_sem,
):
    gr, fs, tp = lax.axis_index("gr"), lax.axis_index("fs"), lax.axis_index("tp")
    other = 1 - tp
    across = (1 - gr, fs, tp)
    across_twin = (1 - gr, fs, other)
    twin = (gr, fs, other)
    expert = fs * 2 + tp
    width = pieces.shape[2]
    hidden_piece = pieces.shape[1] // (2 * n)
    hidden = n * hidden_piece
    shared_piece = shared_mine.shape[1]
    extra = shared_piece // 2
    features = 4 * width
    row_count = tokens_ref.shape[0]
    depth = n // 2
    outer, inner = lax.div(fs, 2), lax.rem(fs, 2)
    beside = (gr, outer * 2 + 1 - inner, tp)
    toward = jnp.where(outer < depth // 2, 1, -1)

    inputs_in = []
    for i, (source, target) in enumerate(
        (
            (tokens_hbm, tokens_ref),
            (routes_hbm, routes_ref),
            (route_weights_hbm, route_weights_ref),
            (gain_hbm, gain_ref),
            (shared_gate_hbm, shared_stage.at[0]),
            (shared_up_hbm, shared_stage.at[1]),
            (shared_down_hbm, shared_stage.at[2]),
        )
    ):
        inputs_in.append(pltpu.make_async_copy(source, target, input_sem.at[i]))
        inputs_in[i].start()
    barrier = pltpu.get_barrier_semaphore()
    for device in (across, across_twin, twin):
        pl.semaphore_signal(barrier, inc=1, device_id=device, device_id_type=MESH)
    for k in range(1, n):
        for t in range(2):
            pl.semaphore_signal(
                barrier, inc=1, device_id=(gr, lax.rem(fs + k, n), t), device_id_type=MESH
            )

    own_start = pl.multiple_of(expert * row_count, row_count)
    few = 16
    inputs_in[0].wait()
    staged = {}
    for t in (0, 1):
        for j, ref in enumerate((gate_hbm, up_hbm, down_hbm)):
            part = pl.ds(t * hidden, hidden)
            staged[j, t] = pltpu.make_async_copy(ref.at[part], stage.at[j, part], stage_sem.at[j, t])
            staged[j, t].start()

    @pl.loop(0, row_count // few)
    def _(i):
        at = pl.multiple_of(i * few, few)
        values = tokens_ref[pl.ds(at, few), :].astype(jnp.float32)
        mean = jnp.mean(values * values, axis=1, keepdims=True)
        normed = (values * lax.rsqrt(mean + epsilon)).astype(jnp.bfloat16)
        rows[pl.ds(own_start + at, few), 0:features] = normed

    for copy in inputs_in[1:]:
        copy.wait()
    number = lax.broadcasted_iota(jnp.int32, (LANES // 2, row_count), 0)
    factors = jnp.zeros(number.shape, jnp.float32)
    for k in range(routes_ref.shape[0]):
        named = routes_ref[k : k + 1, :] == number
        factors = factors + jnp.where(named, route_weights_ref[k : k + 1, :], 0.0)
    high = factors.astype(jnp.bfloat16).astype(jnp.float32)
    both = jnp.concatenate([high, factors - high], axis=0)
    rows[pl.ds(own_start, row_count), features : features + LANES] = both.T.astype(jnp.bfloat16)

    pl.semaphore_wait(barrier, 2 * n + 1)

    def remote(src, dst, send, recv, device):
        return pltpu.make_async_remote_copy(
            src_ref=src,
            dst_ref=dst,
            send_sem=send,
            recv_sem=recv,
            device_id=device,
            device_id_type=MESH,
        )

    def columns(g, t):
        return pl.ds(pl.multiple_of((g * 2 + t) * width, width), width)

    def piece(e):
        return pieces.at[:, pl.ds(pl.multiple_of(e * hidden_piece, 16), hidden_piece), :]

    def portion(t):
        return pieces.at[:, pl.ds(pl.multiple_of(t * hidden, 16), hidden), :]

    def sliced(g, t):
        return weights.at[:, pl.ds(0, hidden), columns(g, t)]

    def slab(source, span):
        start = pl.multiple_of(source * hidden_piece, 16)
        return owned.at[:, pl.ds(start, hidden_piece), span]

    def row_block(source, t):
        start = pl.multiple_of((source * 2 + t) * row_count, row_count)
        return rows.at[pl.ds(start, row_count)]

    late = row_count * 3 // 8
    early = row_count - late

    def row_early(source):
        start = pl.multiple_of((source * 2 + tp) * row_count, row_count)
        return rows.at[pl.ds(start, early)]

    def row_late(source):
        start = pl.multiple_of((source * 2 + tp) * row_count, row_count)
        return rows.at[pl.ds(pl.multiple_of(start + early, 16), late)]

    def nearby(k):
        place = lax.rem(outer + toward * lax.div(k, 2) + depth, depth)
        return place * 2 + jnp.where(lax.rem(k, 2) == 0, inner, 1 - inner)

    half = pl.ds(pl.multiple_of(gr * 2 * width, width), 2 * width)
    far_half = pl.ds(pl.multiple_of((1 - gr) * 2 * width, width), 2 * width)

    def slice_send(index, t, device):
        return remote(
            portion(t), sliced(gr, tp), slice_out_sem.at[index], slice_sem.at[index], device
        )

    def piece_send(d, t):
        return remote(
            piece(d * 2 + t),
            slab(fs, columns(gr, tp)),
            piece_sem.at[d, t],
            weight_sem.at[fs, tp],
            (gr, d, t),
        )

    pair = 2 * hidden_piece

    def guest_send(place):
        start = pl.multiple_of((place * 2 + 1 - inner) * pair, 16)
        spot = pl.ds(place * pair, pair)
        return remote(
            pieces.at[:, pl.ds(start, pair), :],
            guests.at[:, spot, :],
            guest_out_sem.at[place],
            guest_sem.at[place],
            beside,
        )

    fs_beside = outer * 2 + 1 - inner

    def guest(place, t):
        start = pl.multiple_of(place * pair + t * hidden_piece, 16)
        return guests.at[:, pl.ds(start, hidden_piece), :]

    def guest_onward(place, t):
        return remote(
            guest(place, t),
            slab(fs_beside, columns(gr, tp)),
            guest_on_sem.at[place, t],
            weight_sem.at[fs_beside, tp],
            (gr, place * 2 + inner, t),
        )

    guest_local = pltpu.make_async_copy(
        guest(outer, tp), slab(fs_beside, columns(gr, tp)), local_sem.at[0]
    )

    def column_send(source):
        return remote(
            slab(source, half),
            slab(source, half),
            column_out_sem.at[source],
            column_sem.at[source],
            across,
        )

    def row_move(source, send, recv, device):
        return remote(row_block(source, tp), row_block(source, tp), send, recv, device)

    def row_onward(source, step):
        return row_move(
            source,
            row_out_sem.at[source],
            row_sem.at[source],
            (gr, (outer + step) * 2 + inner, tp),
        )

    def row_beside(source, distance):
        block = row_early(source) if distance < depth - 1 else row_block(source, tp)
        return remote(block, block, row_side_sem.at[lax.div(source, 2)], row_sem.at[source], beside)

    def mixed(place, send, step):
        block = row_late(place * 2 + 1 - inner)
        device = (gr, (outer + step) * 2 + inner, tp)
        return remote(block, block, send, mix_sem.at[place], device)

    mix_up = mixed(outer, mix_out_sem.at[outer], 1)
    mix_back = mixed(outer, mix_back_sem.at[0], -1)

    def row_relay(source):
        return row_move(source, row_pair_out_sem.at[source], row_pair_sem.at[source], twin)

    own_up = row_move(fs, row_out_sem.at[fs], row_sem.at[fs], (gr, (outer + 1) * 2 + inner, tp))
    own_back = row_move(fs, row_back_sem.at[0], row_sem.at[fs], (gr, (outer - 1) * 2 + inner, tp))
    own_beside = row_move(fs, row_side_sem.at[outer], row_sem.at[fs], beside)
    own_relay = row_move(fs, row_pair_out_sem.at[fs], row_pair_sem.at[fs], twin)

    def at_distance(distance, action):
        for step in (-1, 1):
            place = outer - step * distance

            @pl.when((place >= 0) & (place < depth))
            def _():
                action(place, step, distance)

    def onward_exists(step):
        return (outer + step >= 0) & (outer + step < depth)

    @pl.when(outer < depth - 1)
    def _():
        own_up.start()

    @pl.when(outer > 0)
    def _():
        own_back.start()

    own_beside.start()
    own_relay.start()
    gain = gain_ref[...]
    for j in range(3):
        value = shared_stage[j] if j == 2 else shared_stage[j] * gain
        shared_mine[j] = value.astype(jnp.bfloat16)
    for t in (0, 1):
        for j in range(3):
            staged[j, t].wait()

            @pl.loop(0, n)
            def _(i):
                at = pl.ds(pl.multiple_of((t * n + i) * hidden_piece, hidden_piece), hidden_piece)
                value = stage[j, at, :] if j == 2 else stage[j, at, :] * gain_ref[...]
                pieces[j, at, :] = value.astype(jnp.bfloat16)

    lane = lax.broadcasted_iota(jnp.int32, select.shape, 0)
    unit = lax.broadcasted_iota(jnp.int32, select.shape, 1)
    first = (jnp.where(lane < LANES // 2, lane, lane - LANES // 2) - tp * n) * hidden_piece
    inside = (unit >= first) & (unit < first + hidden_piece) & (unit < hidden)
    select[...] = jnp.where(inside, 1.0, 0.0).astype(select.dtype)
    shared_far = remote(
        shared_mine, shared.at[:, :, columns(gr, tp)], shared_out_sem.at[0], shared_sem.at[0], across
    )
    shared_far.start()
    slice_far = slice_send(0, tp, across)
    slice_cross = slice_send(1, other, across_twin)
    slice_twin = slice_send(2, other, twin)
    slice_far.start()
    slice_cross.start()
    slice_twin.start()
    shared_twin = remote(
        shared_mine, shared.at[:, :, columns(gr, tp)], shared_out_sem.at[1], shared_sem.at[1], twin
    )
    shared_twin.start()
    twin_piece = piece_send(fs, other)
    twin_piece.start()

    def ship(places):
        for place in places:

            @pl.when(place != outer)
            def _():
                piece_send(place * 2 + inner, 0).start()
                piece_send(place * 2 + inner, 1).start()

    own_slice = pltpu.make_async_copy(portion(tp), sliced(gr, tp), local_sem.at[1])
    own_piece = pltpu.make_async_copy(piece(expert), slab(fs, columns(gr, tp)), local_sem.at[2])
    own_shared = pltpu.make_async_copy(
        shared_mine, shared.at[:, :, columns(gr, tp)], local_sem.at[3]
    )
    locals_ = (own_slice, own_piece, own_shared)
    for copy in locals_:
        copy.start()

    def take_rows(source):
        row_move(source, row_out_sem.at[source], row_sem.at[source], twin).wait_recv()

    def arrive(place, step, distance):
        source = place * 2 + inner
        take_rows(source)

        @pl.when(onward_exists(step))
        def _():
            row_onward(source, step).start()

        row_beside(source, distance).start()
        row_relay(source).start()

    def arrive_mixed(place, step, distance):
        mixed(place, mix_out_sem.at[place], step).wait_recv()
        if distance < depth - 2:

            @pl.when(onward_exists(step))
            def _():
                mixed(place, mix_out_sem.at[place], step).start()

    def arrive_beside(place, step, distance):
        source = place * 2 + 1 - inner
        row_beside(source, distance).wait_recv()
        row_relay(source).start()

    at_distance(1, arrive)
    take_rows(outer * 2 + 1 - inner)

    @pl.when(outer < depth - 1)
    def _():
        mix_up.start()

    @pl.when(outer > 0)
    def _():
        mix_back.start()

    row_relay(outer * 2 + 1 - inner).start()
    for place in range(depth):
        guest_send(place).start()
    for copy in locals_:
        copy.wait()
    far_columns = shared.at[:, :, columns(1 - gr, tp)]
    remote(shared_mine, far_columns, shared_out_sem.at[0], shared_sem.at[0], across).wait_recv()
    shared_relay = remote(far_columns, far_columns, shared_out_sem.at[2], shared_sem.at[2], twin)
    shared_relay.start()
    at_distance(2, arrive)
    ship(range(1, depth - 1))
    at_distance(1, arrive_mixed)
    at_distance(1, arrive_beside)
    at_distance(3, arrive)
    at_distance(2, arrive_mixed)
    ship((0, depth - 1))

    for place in range(depth):
        guest_send(place).wait_recv()

        @pl.when(place != outer)
        def _():
            guest_onward(place, 0).start()
            guest_onward(place, 1).start()

    guest_onward(outer, other).start()
    guest_local.start()
    guest_local.wait()

    def take_twin_piece(source, t):
        remote(
            piece(0),
            slab(source, columns(gr, t)),
            piece_sem.at[fs, other],
            weight_sem.at[source, t],
            twin,
        ).wait_recv()

    take_twin_piece(fs, other)
    column_send(fs).start()
    take_twin_piece(fs_beside, other)
    column_send(fs_beside).start()

    remote(
        shared_mine, shared.at[:, :, columns(gr, other)], shared_out_sem.at[1], shared_sem.at[1], twin
    ).wait_recv()
    last_columns = shared.at[:, :, columns(1 - gr, other)]
    remote(shared_mine, last_columns, shared_out_sem.at[2], shared_sem.at[2], twin).wait_recv()
    tail = pltpu.make_async_copy(
        shared.at[:, pl.ds(pl.multiple_of(tp * extra, extra), extra), :],
        weights.at[:, pl.ds(hidden, extra), :],
        local_sem.at[4],
    )
    tail.start()
    tail.wait()
    remote(portion(tp), sliced(gr, other), slice_out_sem.at[2], slice_sem.at[2], twin).wait_recv()
    remote(portion(tp), sliced(1 - gr, tp), slice_out_sem.at[0], slice_sem.at[0], across).wait_recv()
    remote(
        portion(tp), sliced(1 - gr, other), slice_out_sem.at[1], slice_sem.at[1], across
    ).wait_recv()

    def part_send(k):
        return remote(
            parts.at[k, pl.ds(pl.multiple_of(other * row_count, row_count), row_count), :],
            pair_in.at[k],
            part_sem.at[k],
            part_recv_sem.at[k],
            twin,
        )

    low = outer < depth // 2
    near = jnp.where(low, 1, 2 * depth - 3) - outer
    at_end = (outer == 0) | (outer == depth - 1)

    def place_of(j):
        far = jnp.where(low, depth // 2 + j, depth // 2 - 1 - j)
        return jnp.where(j < depth // 2, far, jnp.where(j == depth - 1, outer, near))

    steps = 2
    span_rows = row_count // steps

    def share(h):
        return pl.ds(h * span_rows, span_rows)

    def side_send(j, h):
        return remote(
            sums.at[2 * j, share(h)],
            side_in.at[j, share(h)],
            side_sem.at[j, h],
            side_recv_sem.at[j, h],
            beside,
        )

    def mate_send(j, h):
        return remote(
            sums.at[2 * j + 1, share(h)],
            mate_in.at[j, share(h)],
            sum_sem.at[j, h],
            mate_sem.at[j, h],
            (gr, near * 2 + inner, tp),
        )

    def sum_send(j, h):
        slot = 1 if j < depth // 2 else 0
        return remote(
            sums.at[2 * j + 1, share(h)],
            sums_in.at[slot, share(h)],
            sum_sem.at[j, h],
            sum_recv_sem.at[slot, h],
            (gr, place_of(j) * 2 + inner, tp),
        )

    chunk = 32

    def add_pair(k, h):
        @pl.loop(0, span_rows // chunk)
        def _(i):
            at = pl.multiple_of(h * span_rows + i * chunk, chunk)
            mine = pl.multiple_of(tp * row_count + at, chunk)
            value = parts[k, pl.ds(mine, chunk), :].astype(jnp.float32)
            value = value + pair_in[k, pl.ds(at, chunk), :].astype(jnp.float32)
            sums[k, pl.ds(at, chunk), :] = value.astype(jnp.bfloat16)

    def await_both(j, h):
        if h == 0:
            part_send(2 * j + 1).wait_recv()
        side_send(j, h).wait_recv()

    def add_both(j, h, mate):
        k = 2 * j + 1

        @pl.loop(0, span_rows // chunk)
        def _(i):
            at = pl.multiple_of(h * span_rows + i * chunk, chunk)
            mine = pl.multiple_of(tp * row_count + at, chunk)
            value = parts[k, pl.ds(mine, chunk), :].astype(jnp.float32)
            value = value + pair_in[k, pl.ds(at, chunk), :].astype(jnp.float32)
            value = value + side_in[j, pl.ds(at, chunk), :].astype(jnp.float32)
            if mate:
                value = value + mate_in[j, pl.ds(at, chunk), :].astype(jnp.float32)
            sums[k, pl.ds(at, chunk), :] = value.astype(jnp.bfloat16)

    def take_weights(source):
        take_twin_piece(source, 0)
        take_twin_piece(source, 1)
        column_send(source).start()

    def pass_far(j, h):
        await_both(j, h)

        @pl.when(at_end)
        def _():
            add_both(j, h, False)
            mate_send(j, h).start()

        @pl.when(jnp.logical_not(at_end))
        def _():
            mate_send(j, h).wait_recv()
            add_both(j, h, True)
            sum_send(j, h).start()

    def pass_near(j):
        for h in range(steps):
            await_both(j, h)
            add_both(j, h, False)
            sum_send(j, h).start()

    @pl.loop(0, n)
    def _(k):
        turn = lax.div(k, 2)
        swapped = jnp.logical_not(at_end) & (turn > 0) & (turn < depth - 1)
        j = jnp.where(swapped, depth - 1 - turn, turn)
        item = 2 * j + lax.rem(k, 2)
        d = place_of(j) * 2 + jnp.where(lax.rem(k, 2) == 0, 1 - inner, inner)

        @pl.when(k == jnp.where(at_end, 0, 4))
        def _():
            at_distance(2, arrive_beside)

        @pl.when(k == 2)
        def _():
            at_distance(3, arrive_beside)

        remote(
            row_block(d, other), row_block(d, other), row_pair_out_sem.at[d], row_pair_sem.at[d], twin
        ).wait_recv()
        block = pl.ds(pl.multiple_of(d * 2 * row_count, 2 * row_count), 2 * row_count)
        inputs = rows[block, 0:features]
        scale = jnp.dot(
            rows[block, features : features + LANES],
            select[...],
            preferred_element_type=jnp.float32,
        )
        gate = contract_rows(inputs, weights[0])
        up = contract_rows(inputs, weights[1])
        position = lax.broadcasted_iota(jnp.int32, gate.shape, 1)
        scale = jnp.where(position < hidden, scale, 1.0)
        units = (gate / (1.0 + jnp.exp(-gate)) * up * scale).astype(jnp.bfloat16)
        for c in range(4):
            span = pl.ds(c * width, width)
            parts[item, :, span] = jnp.dot(
                units, weights[2, :, span], preferred_element_type=jnp.float32
            ).astype(jnp.bfloat16)
        part_send(item).start()

        @pl.when(lax.rem(k, 2) == 1)
        def _():
            part_send(item - 1).wait_recv()
            for h in range(steps):
                add_pair(item - 1, h)
                side_send(j, h).start()

        @pl.when(k == 1)
        def _():
            take_weights(nearby(2))

        @pl.when(k == 2)
        def _():
            take_weights(nearby(4))
            take_weights(nearby(6))

        @pl.when((k > depth) & (k < n - 1))
        def _():
            take_weights(nearby(2 * (k - depth) + 1))

        for h in range(steps):

            @pl.when((k == n - 4 + 2 * h // steps) & at_end)
            def _():
                pass_far(0, h)

    @pl.when(jnp.logical_not(at_end))
    def _():
        pass_near(2)
        take_weights(nearby(n - 1))
        for h in range(steps):
            pass_far(0, h)

    for h in range(steps):
        pass_far(1, h)

    @pl.when(at_end)
    def _():
        take_weights(nearby(n - 1))
        pass_near(2)


    for k in range(n):
        source = nearby(k)
        remote(
            slab(source, far_half),
            slab(source, far_half),
            column_out_sem.at[source],
            column_sem.at[source],
            across,
        ).wait_recv()

    for h in range(steps):
        await_both(depth - 1, h)
        add_both(depth - 1, h, False)
    for h in range(steps):
        for j in range(2):
            remote(
                sums.at[0, share(h)],
                sums_in.at[j, share(h)],
                sum_sem.at[0, 0],
                sum_recv_sem.at[j, h],
                twin,
            ).wait_recv()

        @pl.loop(0, span_rows // chunk)
        def _(i):
            at = pl.ds(pl.multiple_of(h * span_rows + i * chunk, chunk), chunk)
            total = sums[n - 1, at, :].astype(jnp.float32)
            for j in range(2):
                total = total + sums_in[j, at, :].astype(jnp.float32)
            combined_ref[at, :] = total.astype(jnp.bfloat16)

    @pl.when(outer < depth - 1)
    def _():
        own_up.wait_send()
        mix_up.wait_send()

    @pl.when(outer > 0)
    def _():
        own_back.wait_send()
        mix_back.wait_send()

    for copy in (
        own_beside,
        own_relay,
        shared_far,
        slice_far,
        slice_cross,
        slice_twin,
        shared_twin,
        twin_piece,
        shared_relay,
    ):
        copy.wait_send()

    def sent(place, step, distance):
        source = place * 2 + inner

        @pl.when(onward_exists(step))
        def _():
            row_onward(source, step).wait_send()
            if distance < depth - 2:
                mixed(place, mix_out_sem.at[place], step).wait_send()

        row_beside(source, distance).wait_send()

    for distance in range(1, depth):
        at_distance(distance, sent)
    column_send(fs).wait_send()
    for k in range(1, n):
        d = lax.rem(fs + k, n)
        column_send(d).wait_send()
        row_relay(d).wait_send()
    for place in range(depth):
        guest_send(place).wait_send()

        @pl.when(place != outer)
        def _():
            for t in range(2):
                piece_send(place * 2 + inner, t).wait_send()
                guest_onward(place, t).wait_send()

    guest_onward(outer, other).wait_send()
    for k in range(n):
        part_send(k).wait_send()
    for h in range(steps):
        for j in range(depth):
            side_send(j, h).wait_send()
        for j in range(depth - 1):
            sum_send(j, h).wait_send()


def direct_body(
    tokens,
    routes,
    route_weights,
    norm_gain,
    gate_trained,
    up_trained,
    down_trained,
    shared_gate_trained,
    shared_up_trained,
    shared_down_trained,
):
    n = lax.axis_size("fs")
    experts, hidden_piece, width = gate_trained.shape
    row_count, features = tokens.shape
    shared_piece = shared_gate_trained.shape[0]
    stacked = (experts * hidden_piece, width)
    hidden = n * hidden_piece
    hidden_all = hidden + shared_piece // 2
    vmem = pl.BlockSpec(memory_space=pltpu.VMEM)
    hbm = pl.BlockSpec(memory_space=pltpu.HBM)
    kind = jnp.bfloat16
    DMA = pltpu.SemaphoreType.DMA
    combined, owned, shared = pl.pallas_call(
        functools.partial(exchange_kernel, n),
        out_shape=(
            jax.ShapeDtypeStruct((row_count, features), kind),
            jax.ShapeDtypeStruct((3, hidden, features), kind),
            jax.ShapeDtypeStruct((3, shared_piece, features), kind),
        ),
        in_specs=[hbm] * 10,
        out_specs=(vmem,) * 3,
        scratch_shapes=[
            pltpu.VMEM((3, hidden_all, features), kind),
            pltpu.VMEM((experts * row_count, features + LANES), kind),
            pltpu.VMEM((LANES, hidden_all), kind),
            pltpu.VMEM((row_count, features), kind),
            pltpu.VMEM(routes.shape[::-1], jnp.int32),
            pltpu.VMEM(routes.shape[::-1], jnp.float32),
            pltpu.VMEM((1, width), jnp.float32),
            pltpu.VMEM((3, shared_piece, width), jnp.float32),
            pltpu.VMEM((3,) + stacked, jnp.float32),
            pltpu.VMEM((3,) + stacked, kind),
            pltpu.VMEM((3, n * hidden_piece, width), kind),
            pltpu.VMEM((3, shared_piece, width), kind),
            pltpu.VMEM((n, 2 * row_count, features), kind),
            pltpu.VMEM((n, row_count, features), kind),
            pltpu.VMEM((n, row_count, features), kind),
            pltpu.VMEM((n // 2, row_count, features), kind),
            pltpu.VMEM((n // 4, row_count, features), kind),
            pltpu.VMEM((2, row_count, features), kind),
            DMA((5,)),
            DMA((3,)),
            DMA((3,)),
            DMA((n, 2)),
            DMA((n // 2,)),
            DMA((n // 2,)),
            DMA((n // 2, 2)),
            DMA((n, 2)),
            DMA((n,)),
            DMA((n,)),
            DMA((3,)),
            DMA((3,)),
            DMA((n,)),
            DMA((n // 2,)),
            DMA((1,)),
            DMA((n,)),
            DMA((n // 2,)),
            DMA((1,)),
            DMA((n // 2,)),
            DMA((n,)),
            DMA((n,)),
            DMA((n,)),
            DMA((n,)),
            DMA((n // 2, 2)),
            DMA((n // 2, 2)),
            DMA((n // 2 - 1, 2)),
            DMA((n // 4, 2)),
            DMA((2, 2)),
            DMA((3, 2)),
            DMA((7,)),
        ],
        compiler_params=pltpu.CompilerParams(
            collective_id=0, has_side_effects=True, vmem_limit_bytes=48 * 1024 * 1024
        ),
    )(*[
        pltpu.with_memory_space_constraint(array, pltpu.HBM)
        for array in (
            tokens,
            routes.T,
            route_weights.T,
            norm_gain[None, :],
            gate_trained.reshape(stacked),
            up_trained.reshape(stacked),
            down_trained.reshape(stacked),
            shared_gate_trained,
            shared_up_trained,
            shared_down_trained,
        )
    ])
    return settle(combined, owned, shared)


def settle_kernel(combined_ref, owned_ref, shared_ref, combined_out, *refs):
    sems = refs[-1]
    copies = [pltpu.make_async_copy(combined_ref, combined_out, sems.at[6])]
    for j in range(3):
        copies.append(pltpu.make_async_copy(owned_ref.at[j], refs[j].at[0], sems.at[j]))
        copies.append(pltpu.make_async_copy(shared_ref.at[j], refs[3 + j], sems.at[3 + j]))
    for copy in copies:
        copy.start()
    for copy in copies:
        copy.wait()


def settle(combined, owned, shared):
    expert_shape = jax.ShapeDtypeStruct((1,) + owned.shape[1:], owned.dtype)
    shared_shape = jax.ShapeDtypeStruct(shared.shape[1:], shared.dtype)
    return pl.pallas_call(
        settle_kernel,
        out_shape=(jax.ShapeDtypeStruct(combined.shape, combined.dtype),)
        + (expert_shape,) * 3
        + (shared_shape,) * 3,
        in_specs=[pl.BlockSpec(memory_space=pltpu.VMEM)] * 3,
        out_specs=(pl.BlockSpec(memory_space=pltpu.HBM),) * 7,
        scratch_shapes=[pltpu.SemaphoreType.DMA((7,))],
        compiler_params=pltpu.CompilerParams(vmem_limit_bytes=8 * 1024 * 1024),
    )(combined, owned, shared)


def body(*arguments):
    experts = lax.axis_size("fs") * lax.axis_size("tp")
    per_token = arguments[1].shape[1]
    pairs = lax.axis_size("gr") == 2 and lax.axis_size("tp") == 2
    if pairs and lax.axis_size("fs") == 8 and experts <= min(2 * per_token, LANES // 2):
        return direct_body(*arguments)
    return dispatch_body(*arguments)


def solution(mesh):
    in_specs = (
        P(("gr", "fs", "tp"), None),
        P(("gr", "fs", "tp"), None),
        P(("gr", "fs", "tp"), None),
        P(("gr", "tp")),
        P(None, "fs", ("gr", "tp")),
        P(None, "fs", ("gr", "tp")),
        P(None, "fs", ("gr", "tp")),
        P("fs", ("gr", "tp")),
        P("fs", ("gr", "tp")),
        P("fs", ("gr", "tp")),
    )
    out_specs = (
        P(("gr", "fs", "tp"), None),
        P(("fs", "tp"), None, None),
        P(("fs", "tp"), None, None),
        P(("fs", "tp"), None, None),
        P("fs", None),
        P("fs", None),
        P("fs", None),
    )
    return jax.shard_map(body, mesh=mesh, in_specs=in_specs, out_specs=out_specs, check_vma=False)
```

```python
import functools

import jax
import jax.numpy as jnp
from jax import lax
from jax.experimental import pallas as pl
from jax.experimental.pallas import tpu as pltpu
from jax.sharding import PartitionSpec as P

epsilon = 1e-06
LANES = 128
MESH = pl.DeviceIdType.MESH


def contract_rows(inputs, matrix):
    return lax.dot_general(
        inputs, matrix, (((1,), (1,)), ((), ())), preferred_element_type=jnp.float32
    )


def swiglu_rows(inputs, gate_matrix, up_matrix, down_matrix):
    hidden = (
        jax.nn.silu(contract_rows(inputs, gate_matrix)) * contract_rows(inputs, up_matrix)
    ).astype(jnp.bfloat16)
    return jnp.dot(hidden, down_matrix, preferred_element_type=jnp.float32)


def dispatch_body(
    tokens,
    routes,
    route_weights,
    norm_gain,
    gate_trained,
    up_trained,
    down_trained,
    shared_gate_trained,
    shared_up_trained,
    shared_down_trained,
):
    gain_row = norm_gain[None, None, :]
    stacked = jnp.stack(
        [gate_trained * gain_row, up_trained * gain_row, down_trained], axis=1
    ).astype(jnp.bfloat16)
    halves = lax.all_to_all(
        lax.all_to_all(stacked[:, :, :, None, :], "fs", split_axis=0, concat_axis=2, tiled=True),
        "tp",
        split_axis=0,
        concat_axis=3,
        tiled=True,
    )
    owned = lax.all_gather(halves[:, :, :, None], "gr", axis=3, tiled=True)
    owned = owned.reshape(owned.shape[0], 3, owned.shape[2], -1)
    expert_gate = owned[:, 0]
    expert_up = owned[:, 1]
    expert_down = owned[:, 2]
    shared_gain = norm_gain[None, :]
    shared_stack = jnp.stack(
        [shared_gate_trained * shared_gain, shared_up_trained * shared_gain, shared_down_trained],
        axis=0,
    ).astype(jnp.bfloat16)
    shared_whole = lax.all_gather(shared_stack, ("gr", "tp"), axis=2, tiled=True)
    shared_gate = shared_whole[0]
    shared_up = shared_whole[1]
    shared_down = shared_whole[2]
    values = tokens.astype(jnp.float32)
    normed = (
        values * lax.rsqrt(jnp.mean(values * values, axis=1, keepdims=True) + epsilon)
    ).astype(jnp.bfloat16)
    row_count, features = normed.shape
    per_token = routes.shape[1]
    shared_out = swiglu_rows(
        normed,
        lax.all_gather(shared_gate, "fs", axis=0, tiled=True),
        lax.all_gather(shared_up, "fs", axis=0, tiled=True),
        lax.all_gather(shared_down, "fs", axis=0, tiled=True),
    )
    experts = lax.axis_size("fs") * lax.axis_size("tp")
    capacity = max(2, 3 * row_count * per_token // (2 * experts))
    chosen = routes.reshape(-1)
    onehot = (chosen[:, None] == jnp.arange(experts, dtype=jnp.int32)[None, :]).astype(jnp.int32)
    position = jnp.sum((jnp.cumsum(onehot, axis=0) - onehot) * onehot, axis=1)
    target = chosen * capacity + position
    source = (
        jnp.full((experts * capacity,), row_count, jnp.int32)
        .at[target]
        .set(jnp.arange(row_count * per_token, dtype=jnp.int32) // per_token)
    )
    padded = jnp.concatenate([normed, jnp.zeros((1, features), jnp.bfloat16)], axis=0)
    outgoing = padded[source].reshape(experts, capacity, features)
    arrived = lax.all_to_all(outgoing, ("fs", "tp"), split_axis=0, concat_axis=0, tiled=True)
    item_count = arrived.shape[1]
    result = swiglu_rows(
        arrived.reshape(-1, features), expert_gate[0], expert_up[0], expert_down[0]
    )
    result = result.astype(jnp.bfloat16).reshape(experts, item_count, features)
    returned = lax.all_to_all(result, ("fs", "tp"), split_axis=0, concat_axis=0, tiled=True)
    picked = returned.reshape(experts * capacity, features)[target].astype(jnp.float32)
    picked = picked.reshape(row_count, per_token, features)
    routed = jnp.sum(picked * route_weights[:, :, None], axis=1)
    combined = (routed + shared_out).astype(jnp.bfloat16)
    return (combined, expert_gate, expert_up, expert_down, shared_gate, shared_up, shared_down)


class Both:
    def __init__(self, *copies):
        self.copies = copies

    def start(self):
        for copy in self.copies:
            copy.start()

    def wait_recv(self):
        for copy in self.copies:
            copy.wait_recv()

    def wait_send(self):
        for copy in self.copies:
            copy.wait_send()


def exchange_kernel(
    n,
    tokens_hbm,
    routes_hbm,
    route_weights_hbm,
    gain_hbm,
    gate_hbm,
    up_hbm,
    down_hbm,
    shared_gate_hbm,
    shared_up_hbm,
    shared_down_hbm,
    combined_ref,
    owned,
    shared,
    weights,
    rows,
    table,
    select,
    tokens_ref,
    routes_ref,
    route_weights_ref,
    gain_ref,
    shared_stage,
    stage,
    pieces,
    guests,
    shared_mine,
    parts,
    pair_in,
    sums,
    side_in,
    mate_in,
    sums_in,
    local_sem,
    slice_out_sem,
    slice_sem,
    piece_sem,
    guest_out_sem,
    guest_sem,
    guest_on_sem,
    weight_sem,
    column_out_sem,
    column_sem,
    shared_out_sem,
    shared_sem,
    row_out_sem,
    row_side_sem,
    row_back_sem,
    row_sem,
    mix_out_sem,
    mix_back_sem,
    mix_sem,
    row_pair_out_sem,
    row_pair_sem,
    part_sem,
    part_recv_sem,
    side_sem,
    side_recv_sem,
    sum_sem,
    mate_sem,
    sum_recv_sem,
    stage_sem,
    input_sem,
):
    gr, fs, tp = lax.axis_index("gr"), lax.axis_index("fs"), lax.axis_index("tp")
    other = 1 - tp
    across = (1 - gr, fs, tp)
    across_twin = (1 - gr, fs, other)
    twin = (gr, fs, other)
    expert = fs * 2 + tp
    width = pieces.shape[2]
    hidden_piece = pieces.shape[1] // (2 * n)
    hidden = n * hidden_piece
    shared_piece = shared_mine.shape[1]
    extra = shared_piece // 2
    features = 4 * width
    row_count = tokens_ref.shape[0]
    depth = n // 2
    outer, inner = lax.div(fs, 2), lax.rem(fs, 2)
    beside = (gr, outer * 2 + 1 - inner, tp)
    toward = jnp.where(outer < depth // 2, 1, -1)

    inputs_in = []
    for i, (source, target) in enumerate(
        (
            (tokens_hbm, tokens_ref),
            (routes_hbm, routes_ref),
            (route_weights_hbm, route_weights_ref),
            (gain_hbm, gain_ref),
            (shared_gate_hbm, shared_stage.at[0]),
            (shared_up_hbm, shared_stage.at[1]),
            (shared_down_hbm, shared_stage.at[2]),
        )
    ):
        inputs_in.append(pltpu.make_async_copy(source, target, input_sem.at[i]))
        inputs_in[i].start()
    barrier = pltpu.get_barrier_semaphore()
    for device in (across, across_twin, twin):
        pl.semaphore_signal(barrier, inc=1, device_id=device, device_id_type=MESH)
    for k in range(1, n):
        for t in range(2):
            pl.semaphore_signal(
                barrier, inc=1, device_id=(gr, lax.rem(fs + k, n), t), device_id_type=MESH
            )

    own_start = pl.multiple_of(expert * row_count, row_count)
    few = 16
    inputs_in[0].wait()
    staged = {}
    for t in (0, 1):
        for j, ref in enumerate((gate_hbm, up_hbm, down_hbm)):
            part = pl.ds(t * hidden, hidden)
            staged[j, t] = pltpu.make_async_copy(ref.at[part], stage.at[j, part], stage_sem.at[j, t])
            staged[j, t].start()

    @pl.loop(0, row_count // few)
    def _(i):
        at = pl.multiple_of(i * few, few)
        values = tokens_ref[pl.ds(at, few), :].astype(jnp.float32)
        mean = jnp.mean(values * values, axis=1, keepdims=True)
        normed = (values * lax.rsqrt(mean + epsilon)).astype(jnp.bfloat16)
        rows[pl.ds(own_start + at, few), :] = normed

    for copy in inputs_in[1:]:
        copy.wait()
    number = lax.broadcasted_iota(jnp.int32, (2 * n, row_count), 0)
    factors = jnp.zeros(number.shape, jnp.float32)
    for k in range(routes_ref.shape[0]):
        named = routes_ref[k : k + 1, :] == number
        factors = factors + jnp.where(named, route_weights_ref[k : k + 1, :], 0.0)
    high = factors.astype(jnp.bfloat16).astype(jnp.float32)
    both = jnp.concatenate([high, factors - high], axis=0)
    table[expert] = both.astype(jnp.bfloat16)

    pl.semaphore_wait(barrier, 2 * n + 1)

    def remote(src, dst, send, recv, device):
        return pltpu.make_async_remote_copy(
            src_ref=src,
            dst_ref=dst,
            send_sem=send,
            recv_sem=recv,
            device_id=device,
            device_id_type=MESH,
        )

    def columns(g, t):
        return pl.ds(pl.multiple_of((g * 2 + t) * width, width), width)

    def piece(e):
        return pieces.at[:, pl.ds(pl.multiple_of(e * hidden_piece, 16), hidden_piece), :]

    def portion(t):
        return pieces.at[:, pl.ds(pl.multiple_of(t * hidden, 16), hidden), :]

    def sliced(g, t):
        return weights.at[:, pl.ds(0, hidden), columns(g, t)]

    def slab(source, span):
        start = pl.multiple_of(source * hidden_piece, 16)
        return owned.at[:, pl.ds(start, hidden_piece), span]

    def row_block(source, t):
        start = pl.multiple_of((source * 2 + t) * row_count, row_count)
        return rows.at[pl.ds(start, row_count)]

    late = row_count // 4
    early = row_count - late

    def row_early(source):
        start = pl.multiple_of((source * 2 + tp) * row_count, row_count)
        return rows.at[pl.ds(start, early)]

    def row_late(source):
        start = pl.multiple_of((source * 2 + tp) * row_count, row_count)
        return rows.at[pl.ds(pl.multiple_of(start + early, 16), late)]

    def nearby(k):
        place = lax.rem(outer + toward * lax.div(k, 2) + depth, depth)
        return place * 2 + jnp.where(lax.rem(k, 2) == 0, inner, 1 - inner)

    half = pl.ds(pl.multiple_of(gr * 2 * width, width), 2 * width)
    far_half = pl.ds(pl.multiple_of((1 - gr) * 2 * width, width), 2 * width)

    def slice_send(index, t, device):
        return remote(
            portion(t), sliced(gr, tp), slice_out_sem.at[index], slice_sem.at[index], device
        )

    def piece_send(d, t):
        return remote(
            piece(d * 2 + t),
            slab(fs, columns(gr, tp)),
            piece_sem.at[d, t],
            weight_sem.at[fs, tp],
            (gr, d, t),
        )

    pair = 2 * hidden_piece

    low = outer < depth // 2
    near = jnp.where(low, 1, 2 * depth - 3) - outer
    at_end = (outer == 0) | (outer == depth - 1)

    def direct(place, t):
        return False

    def unless(condition, action):
        if condition is False:
            action()
        else:
            pl.when(jnp.logical_not(condition))(action)

    def guest_send(place, t):
        e = (place * 2 + 1 - inner) * 2 + t
        spot = pl.ds(place * pair + t * hidden_piece, hidden_piece)
        return remote(
            piece(e),
            guests.at[:, spot, :],
            guest_out_sem.at[place, t],
            guest_sem.at[place, t],
            beside,
        )

    fs_beside = outer * 2 + 1 - inner

    def guest(place, t):
        start = pl.multiple_of(place * pair + t * hidden_piece, 16)
        return guests.at[:, pl.ds(start, hidden_piece), :]

    def guest_onward(place, t):
        return remote(
            guest(place, t),
            slab(fs_beside, columns(gr, tp)),
            guest_on_sem.at[place, t],
            weight_sem.at[fs_beside, tp],
            (gr, place * 2 + inner, t),
        )

    guest_local = pltpu.make_async_copy(
        guest(outer, tp), slab(fs_beside, columns(gr, tp)), local_sem.at[0]
    )

    def column_send(source):
        return remote(
            slab(source, half),
            slab(source, half),
            column_out_sem.at[source],
            column_sem.at[source],
            across,
        )

    def with_table(block, source, t, send, recv, device):
        entry = table.at[source * 2 + t]
        return Both(
            remote(block, block, send.at[0], recv.at[0], device),
            remote(entry, entry, send.at[1], recv.at[1], device),
        )

    def row_move(source, send, recv, device):
        return with_table(row_block(source, tp), source, tp, send, recv, device)

    def row_onward(source, step):
        return row_move(
            source,
            row_out_sem.at[source],
            row_sem.at[source],
            (gr, (outer + step) * 2 + inner, tp),
        )

    def row_beside(source, distance):
        block = row_early(source) if distance < depth - 1 else row_block(source, tp)
        return with_table(
            block, source, tp, row_side_sem.at[lax.div(source, 2)], row_sem.at[source], beside
        )

    def mixed(place, send, step):
        block = row_late(place * 2 + 1 - inner)
        device = (gr, (outer + step) * 2 + inner, tp)
        return remote(block, block, send, mix_sem.at[place], device)

    mix_up = mixed(outer, mix_out_sem.at[outer], 1)
    mix_back = mixed(outer, mix_back_sem.at[0], -1)

    def row_relay(source):
        return row_move(source, row_pair_out_sem.at[source], row_pair_sem.at[source], twin)

    own_up = row_move(fs, row_out_sem.at[fs], row_sem.at[fs], (gr, (outer + 1) * 2 + inner, tp))
    own_back = row_move(fs, row_back_sem.at[0], row_sem.at[fs], (gr, (outer - 1) * 2 + inner, tp))
    own_beside = row_move(fs, row_side_sem.at[outer], row_sem.at[fs], beside)
    own_relay = row_move(fs, row_pair_out_sem.at[fs], row_pair_sem.at[fs], twin)

    def at_distance(distance, action):
        for step in (-1, 1):
            place = outer - step * distance

            @pl.when((place >= 0) & (place < depth))
            def _():
                action(place, step, distance)

    def onward_exists(step):
        return (outer + step >= 0) & (outer + step < depth)

    @pl.when(outer < depth - 1)
    def _():
        own_up.start()

    @pl.when(outer > 0)
    def _():
        own_back.start()

    own_beside.start()
    own_relay.start()
    gain = gain_ref[...]
    for j in range(3):
        value = shared_stage[j] if j == 2 else shared_stage[j] * gain
        shared_mine[j] = value.astype(jnp.bfloat16)
    for t in (0, 1):
        for j in range(3):
            staged[j, t].wait()

            @pl.loop(0, n)
            def _(i):
                at = pl.ds(pl.multiple_of((t * n + i) * hidden_piece, hidden_piece), hidden_piece)
                value = stage[j, at, :] if j == 2 else stage[j, at, :] * gain_ref[...]
                pieces[j, at, :] = value.astype(jnp.bfloat16)

    lane = lax.broadcasted_iota(jnp.int32, select.shape, 0)
    unit = lax.broadcasted_iota(jnp.int32, select.shape, 1)
    first = (jnp.where(lane < 2 * n, lane, lane - 2 * n) - tp * n) * hidden_piece
    inside = (unit >= first) & (unit < first + hidden_piece) & (unit < hidden)
    select[...] = jnp.where(inside, 1.0, 0.0).astype(select.dtype)
    shared_far = remote(
        shared_mine, shared.at[:, :, columns(gr, tp)], shared_out_sem.at[0], shared_sem.at[0], across
    )
    shared_far.start()
    slice_far = slice_send(0, tp, across)
    slice_cross = slice_send(1, other, across_twin)
    slice_twin = slice_send(2, other, twin)
    slice_far.start()
    slice_cross.start()
    slice_twin.start()
    shared_twin = remote(
        shared_mine, shared.at[:, :, columns(gr, tp)], shared_out_sem.at[1], shared_sem.at[1], twin
    )
    shared_twin.start()
    twin_piece = piece_send(fs, other)
    twin_piece.start()

    def ship(places):
        for place in places:

            @pl.when(place != outer)
            def _():
                piece_send(place * 2 + inner, 0).start()
                piece_send(place * 2 + inner, 1).start()

    own_slice = pltpu.make_async_copy(portion(tp), sliced(gr, tp), local_sem.at[1])
    own_piece = pltpu.make_async_copy(piece(expert), slab(fs, columns(gr, tp)), local_sem.at[2])
    own_shared = pltpu.make_async_copy(
        shared_mine, shared.at[:, :, columns(gr, tp)], local_sem.at[3]
    )
    locals_ = (own_slice, own_piece, own_shared)
    for copy in locals_:
        copy.start()

    def take_rows(source):
        row_move(source, row_out_sem.at[source], row_sem.at[source], twin).wait_recv()

    def arrive(place, step, distance):
        source = place * 2 + inner
        take_rows(source)

        @pl.when(onward_exists(step))
        def _():
            row_onward(source, step).start()

        row_beside(source, distance).start()
        row_relay(source).start()

    def arrive_mixed(place, step, distance):
        mixed(place, mix_out_sem.at[place], step).wait_recv()
        if distance < depth - 2:

            @pl.when(onward_exists(step))
            def _():
                mixed(place, mix_out_sem.at[place], step).start()

    def arrive_beside(place, step, distance):
        source = place * 2 + 1 - inner
        row_beside(source, distance).wait_recv()
        row_relay(source).start()

    at_distance(1, arrive)
    take_rows(outer * 2 + 1 - inner)

    @pl.when(outer < depth - 1)
    def _():
        mix_up.start()

    @pl.when(outer > 0)
    def _():
        mix_back.start()

    row_relay(outer * 2 + 1 - inner).start()
    for place in range(depth):
        for t in range(2):
            unless(direct(place, t), guest_send(place, t).start)
    for copy in locals_:
        copy.wait()
    far_columns = shared.at[:, :, columns(1 - gr, tp)]
    remote(shared_mine, far_columns, shared_out_sem.at[0], shared_sem.at[0], across).wait_recv()
    shared_relay = remote(far_columns, far_columns, shared_out_sem.at[2], shared_sem.at[2], twin)
    shared_relay.start()
    at_distance(2, arrive)
    ship(range(1, depth - 1))

    at_distance(1, arrive_mixed)
    at_distance(1, arrive_beside)
    at_distance(3, arrive)
    at_distance(2, arrive_mixed)
    ship((0, depth - 1))

    for place in range(depth):
        for t in range(2):

            def onward(place=place, t=t):
                guest_send(place, t).wait_recv()

                @pl.when(place != outer)
                def _():
                    guest_onward(place, t).start()

            unless(direct(place, t), onward)

    guest_onward(outer, other).start()
    guest_local.start()
    guest_local.wait()

    def take_twin_piece(source, t):
        remote(
            piece(0),
            slab(source, columns(gr, t)),
            piece_sem.at[fs, other],
            weight_sem.at[source, t],
            twin,
        ).wait_recv()

    take_twin_piece(fs, other)
    column_send(fs).start()
    take_twin_piece(fs_beside, other)
    column_send(fs_beside).start()

    remote(
        shared_mine, shared.at[:, :, columns(gr, other)], shared_out_sem.at[1], shared_sem.at[1], twin
    ).wait_recv()
    last_columns = shared.at[:, :, columns(1 - gr, other)]
    remote(shared_mine, last_columns, shared_out_sem.at[2], shared_sem.at[2], twin).wait_recv()
    tail = pltpu.make_async_copy(
        shared.at[:, pl.ds(pl.multiple_of(tp * extra, extra), extra), :],
        weights.at[:, pl.ds(hidden, extra), :],
        local_sem.at[4],
    )
    tail.start()
    tail.wait()
    remote(portion(tp), sliced(gr, other), slice_out_sem.at[2], slice_sem.at[2], twin).wait_recv()
    remote(portion(tp), sliced(1 - gr, tp), slice_out_sem.at[0], slice_sem.at[0], across).wait_recv()
    remote(
        portion(tp), sliced(1 - gr, other), slice_out_sem.at[1], slice_sem.at[1], across
    ).wait_recv()

    def part_send(k):
        return remote(
            parts.at[k, pl.ds(pl.multiple_of(other * row_count, row_count), row_count), :],
            pair_in.at[k],
            part_sem.at[k],
            part_recv_sem.at[k],
            twin,
        )

    def place_of(j):
        far = jnp.where(low, depth // 2 + j, depth // 2 - 1 - j)
        return jnp.where(j < depth // 2, far, jnp.where(j == depth - 1, outer, near))

    steps = 2
    span_rows = row_count // steps

    def share(h):
        return pl.ds(h * span_rows, span_rows)

    def side_send(j, h):
        return remote(
            sums.at[2 * j, share(h)],
            side_in.at[j, share(h)],
            side_sem.at[j, h],
            side_recv_sem.at[j, h],
            beside,
        )

    def mate_send(j, h):
        return remote(
            sums.at[2 * j + 1, share(h)],
            mate_in.at[j, share(h)],
            sum_sem.at[j, h],
            mate_sem.at[j, h],
            (gr, near * 2 + inner, tp),
        )

    def sum_send(j, h):
        slot = 1 if j < depth // 2 else 0
        return remote(
            sums.at[2 * j + 1, share(h)],
            sums_in.at[slot, share(h)],
            sum_sem.at[j, h],
            sum_recv_sem.at[slot, h],
            (gr, place_of(j) * 2 + inner, tp),
        )

    chunk = 32

    def add_pair(k, h):
        @pl.loop(0, span_rows // chunk)
        def _(i):
            at = pl.multiple_of(h * span_rows + i * chunk, chunk)
            mine = pl.multiple_of(tp * row_count + at, chunk)
            value = parts[k, pl.ds(mine, chunk), :].astype(jnp.float32)
            value = value + pair_in[k, pl.ds(at, chunk), :].astype(jnp.float32)
            sums[k, pl.ds(at, chunk), :] = value.astype(jnp.bfloat16)

    def await_both(j, h):
        if h == 0:
            part_send(2 * j + 1).wait_recv()
        side_send(j, h).wait_recv()

    def add_both(j, h, mate):
        k = 2 * j + 1

        @pl.loop(0, span_rows // chunk)
        def _(i):
            at = pl.multiple_of(h * span_rows + i * chunk, chunk)
            mine = pl.multiple_of(tp * row_count + at, chunk)
            value = parts[k, pl.ds(mine, chunk), :].astype(jnp.float32)
            value = value + pair_in[k, pl.ds(at, chunk), :].astype(jnp.float32)
            value = value + side_in[j, pl.ds(at, chunk), :].astype(jnp.float32)
            if mate:
                value = value + mate_in[j, pl.ds(at, chunk), :].astype(jnp.float32)
            sums[k, pl.ds(at, chunk), :] = value.astype(jnp.bfloat16)

    def take_weights(source):
        take_twin_piece(source, 0)
        take_twin_piece(source, 1)
        column_send(source).start()

    def pass_far(j, h):
        await_both(j, h)

        @pl.when(at_end)
        def _():
            add_both(j, h, False)
            mate_send(j, h).start()

        @pl.when(jnp.logical_not(at_end))
        def _():
            mate_send(j, h).wait_recv()
            add_both(j, h, True)
            sum_send(j, h).start()

    def pass_near(j):
        for h in range(steps):
            await_both(j, h)
            add_both(j, h, False)
            sum_send(j, h).start()

    @pl.loop(0, n)
    def _(k):
        turn = lax.div(k, 2)
        swapped = jnp.logical_not(at_end) & (turn > 0) & (turn < depth - 1)
        j = jnp.where(swapped, depth - 1 - turn, turn)
        item = 2 * j + lax.rem(k, 2)
        d = place_of(j) * 2 + jnp.where(lax.rem(k, 2) == 0, 1 - inner, inner)

        @pl.when(k == jnp.where(at_end, 0, 4))
        def _():
            at_distance(2, arrive_beside)

        @pl.when(k == 2)
        def _():
            at_distance(3, arrive_beside)

        with_table(
            row_block(d, other), d, other, row_pair_out_sem.at[d], row_pair_sem.at[d], twin
        ).wait_recv()
        block = pl.ds(pl.multiple_of(d * 2 * row_count, 2 * row_count), 2 * row_count)
        inputs = rows[block, :]
        entries = [table[d * 2 + t].astype(jnp.float32).T.astype(jnp.bfloat16) for t in range(2)]
        scale = jnp.dot(
            jnp.concatenate(entries, axis=0), select[...], preferred_element_type=jnp.float32
        )
        gate = contract_rows(inputs, weights[0])
        up = contract_rows(inputs, weights[1])
        position = lax.broadcasted_iota(jnp.int32, gate.shape, 1)
        scale = jnp.where(position < hidden, scale, 1.0)
        units = (gate / (1.0 + jnp.exp(-gate)) * up * scale).astype(jnp.bfloat16)
        for c in range(4):
            span = pl.ds(c * width, width)
            parts[item, :, span] = jnp.dot(
                units, weights[2, :, span], preferred_element_type=jnp.float32
            ).astype(jnp.bfloat16)
        part_send(item).start()

        @pl.when(lax.rem(k, 2) == 1)
        def _():
            part_send(item - 1).wait_recv()
            for h in range(steps):
                add_pair(item - 1, h)
                side_send(j, h).start()

        @pl.when(k == 1)
        def _():
            take_weights(nearby(2))

        @pl.when(k == 2)
        def _():
            take_weights(nearby(4))
            take_weights(nearby(6))

        for h in range(steps):

            @pl.when((k == n - 5 + 2 * h // steps) & at_end)
            def _():
                pass_far(0, h)

        @pl.when((k > depth) & (k < n - 1))
        def _():
            take_weights(nearby(2 * (k - depth) + 1))


    @pl.when(jnp.logical_not(at_end))
    def _():
        pass_near(2)
        take_weights(nearby(n - 1))
        for h in range(steps):
            pass_far(0, h)

    for h in range(steps):
        pass_far(1, h)

    @pl.when(at_end)
    def _():
        take_weights(nearby(n - 1))
        pass_near(2)


    for k in range(n):
        source = nearby(k)
        remote(
            slab(source, far_half),
            slab(source, far_half),
            column_out_sem.at[source],
            column_sem.at[source],
            across,
        ).wait_recv()

    for h in range(steps):
        await_both(depth - 1, h)
        add_both(depth - 1, h, False)
    for h in range(steps):
        for j in range(2):
            remote(
                sums.at[0, share(h)],
                sums_in.at[j, share(h)],
                sum_sem.at[0, 0],
                sum_recv_sem.at[j, h],
                twin,
            ).wait_recv()

        @pl.loop(0, span_rows // chunk)
        def _(i):
            at = pl.ds(pl.multiple_of(h * span_rows + i * chunk, chunk), chunk)
            total = sums[n - 1, at, :].astype(jnp.float32)
            for j in range(2):
                total = total + sums_in[j, at, :].astype(jnp.float32)
            combined_ref[at, :] = total.astype(jnp.bfloat16)

    @pl.when(outer < depth - 1)
    def _():
        own_up.wait_send()
        mix_up.wait_send()

    @pl.when(outer > 0)
    def _():
        own_back.wait_send()
        mix_back.wait_send()

    for copy in (
        own_beside,
        own_relay,
        shared_far,
        slice_far,
        slice_cross,
        slice_twin,
        shared_twin,
        twin_piece,
        shared_relay,
    ):
        copy.wait_send()

    def sent(place, step, distance):
        source = place * 2 + inner

        @pl.when(onward_exists(step))
        def _():
            row_onward(source, step).wait_send()
            if distance < depth - 2:
                mixed(place, mix_out_sem.at[place], step).wait_send()

        row_beside(source, distance).wait_send()

    for distance in range(1, depth):
        at_distance(distance, sent)
    column_send(fs).wait_send()
    for k in range(1, n):
        d = lax.rem(fs + k, n)
        column_send(d).wait_send()
        row_relay(d).wait_send()
    for place in range(depth):
        for t in range(2):

            def done(place=place, t=t):
                guest_send(place, t).wait_send()

                @pl.when(place != outer)
                def _():
                    guest_onward(place, t).wait_send()

            unless(direct(place, t), done)

            @pl.when(place != outer)
            def _():
                piece_send(place * 2 + inner, t).wait_send()

    guest_onward(outer, other).wait_send()

    for k in range(n):
        part_send(k).wait_send()
    for h in range(steps):
        for j in range(depth):
            side_send(j, h).wait_send()
        for j in range(depth - 1):
            sum_send(j, h).wait_send()


def direct_body(
    tokens,
    routes,
    route_weights,
    norm_gain,
    gate_trained,
    up_trained,
    down_trained,
    shared_gate_trained,
    shared_up_trained,
    shared_down_trained,
):
    n = lax.axis_size("fs")
    experts, hidden_piece, width = gate_trained.shape
    row_count, features = tokens.shape
    shared_piece = shared_gate_trained.shape[0]
    stacked = (experts * hidden_piece, width)
    hidden = n * hidden_piece
    hidden_all = hidden + shared_piece // 2
    vmem = pl.BlockSpec(memory_space=pltpu.VMEM)
    hbm = pl.BlockSpec(memory_space=pltpu.HBM)
    kind = jnp.bfloat16
    DMA = pltpu.SemaphoreType.DMA
    combined, owned, shared = pl.pallas_call(
        functools.partial(exchange_kernel, n),
        out_shape=(
            jax.ShapeDtypeStruct((row_count, features), kind),
            jax.ShapeDtypeStruct((3, hidden, features), kind),
            jax.ShapeDtypeStruct((3, shared_piece, features), kind),
        ),
        in_specs=[hbm] * 10,
        out_specs=(vmem,) * 3,
        scratch_shapes=[
            pltpu.VMEM((3, hidden_all, features), kind),
            pltpu.VMEM((experts * row_count, features), kind),
            pltpu.VMEM((experts, 2 * experts, row_count), kind),
            pltpu.VMEM((2 * experts, hidden_all), kind),
            pltpu.VMEM((row_count, features), kind),
            pltpu.VMEM(routes.shape[::-1], jnp.int32),
            pltpu.VMEM(routes.shape[::-1], jnp.float32),
            pltpu.VMEM((1, width), jnp.float32),
            pltpu.VMEM((3, shared_piece, width), jnp.float32),
            pltpu.VMEM((3,) + stacked, jnp.float32),
            pltpu.VMEM((3,) + stacked, kind),
            pltpu.VMEM((3, n * hidden_piece, width), kind),
            pltpu.VMEM((3, shared_piece, width), kind),
            pltpu.VMEM((n, 2 * row_count, features), kind),
            pltpu.VMEM((n, row_count, features), kind),
            pltpu.VMEM((n, row_count, features), kind),
            pltpu.VMEM((n // 2, row_count, features), kind),
            pltpu.VMEM((n // 4, row_count, features), kind),
            pltpu.VMEM((2, row_count, features), kind),
            DMA((5,)),
            DMA((3,)),
            DMA((3,)),
            DMA((n, 2)),
            DMA((n // 2, 2)),
            DMA((n // 2, 2)),
            DMA((n // 2, 2)),
            DMA((n, 2)),
            DMA((n,)),
            DMA((n,)),
            DMA((3,)),
            DMA((3,)),
            DMA((n, 2)),
            DMA((n // 2, 2)),
            DMA((1, 2)),
            DMA((n, 2)),
            DMA((n // 2,)),
            DMA((1,)),
            DMA((n // 2,)),
            DMA((n, 2)),
            DMA((n, 2)),
            DMA((n,)),
            DMA((n,)),
            DMA((n // 2, 2)),
            DMA((n // 2, 2)),
            DMA((n // 2 - 1, 2)),
            DMA((n // 4, 2)),
            DMA((2, 2)),
            DMA((3, 2)),
            DMA((7,)),
        ],
        compiler_params=pltpu.CompilerParams(
            collective_id=0, has_side_effects=True, vmem_limit_bytes=48 * 1024 * 1024
        ),
    )(*[
        pltpu.with_memory_space_constraint(array, pltpu.HBM)
        for array in (
            tokens,
            routes.T,
            route_weights.T,
            norm_gain[None, :],
            gate_trained.reshape(stacked),
            up_trained.reshape(stacked),
            down_trained.reshape(stacked),
            shared_gate_trained,
            shared_up_trained,
            shared_down_trained,
        )
    ])
    return settle(combined, owned, shared)


def settle_kernel(combined_ref, owned_ref, shared_ref, combined_out, *refs):
    sems = refs[-1]
    copies = [pltpu.make_async_copy(combined_ref, combined_out, sems.at[6])]
    for j in range(3):
        copies.append(pltpu.make_async_copy(owned_ref.at[j], refs[j].at[0], sems.at[j]))
        copies.append(pltpu.make_async_copy(shared_ref.at[j], refs[3 + j], sems.at[3 + j]))
    for copy in copies:
        copy.start()
    for copy in copies:
        copy.wait()


def settle(combined, owned, shared):
    expert_shape = jax.ShapeDtypeStruct((1,) + owned.shape[1:], owned.dtype)
    shared_shape = jax.ShapeDtypeStruct(shared.shape[1:], shared.dtype)
    return pl.pallas_call(
        settle_kernel,
        out_shape=(jax.ShapeDtypeStruct(combined.shape, combined.dtype),)
        + (expert_shape,) * 3
        + (shared_shape,) * 3,
        in_specs=[pl.BlockSpec(memory_space=pltpu.VMEM)] * 3,
        out_specs=(pl.BlockSpec(memory_space=pltpu.HBM),) * 7,
        scratch_shapes=[pltpu.SemaphoreType.DMA((7,))],
        compiler_params=pltpu.CompilerParams(vmem_limit_bytes=8 * 1024 * 1024),
    )(combined, owned, shared)


def body(*arguments):
    experts = lax.axis_size("fs") * lax.axis_size("tp")
    per_token = arguments[1].shape[1]
    pairs = lax.axis_size("gr") == 2 and lax.axis_size("tp") == 2
    if pairs and lax.axis_size("fs") == 8 and experts <= min(2 * per_token, LANES // 2):
        return direct_body(*arguments)
    return dispatch_body(*arguments)


def solution(mesh):
    in_specs = (
        P(("gr", "fs", "tp"), None),
        P(("gr", "fs", "tp"), None),
        P(("gr", "fs", "tp"), None),
        P(("gr", "tp")),
        P(None, "fs", ("gr", "tp")),
        P(None, "fs", ("gr", "tp")),
        P(None, "fs", ("gr", "tp")),
        P("fs", ("gr", "tp")),
        P("fs", ("gr", "tp")),
        P("fs", ("gr", "tp")),
    )
    out_specs = (
        P(("gr", "fs", "tp"), None),
        P(("fs", "tp"), None, None),
        P(("fs", "tp"), None, None),
        P(("fs", "tp"), None, None),
        P("fs", None),
        P("fs", None),
        P("fs", None),
    )
    return jax.shard_map(body, mesh=mesh, in_specs=in_specs, out_specs=out_specs, check_vma=False)
```

```python
import functools

import jax
import jax.numpy as jnp
from jax import lax
from jax.experimental import pallas as pl
from jax.experimental.pallas import tpu as pltpu
from jax.sharding import PartitionSpec as P

epsilon = 1e-06
LANES = 128
MESH = pl.DeviceIdType.MESH


def contract_rows(inputs, matrix):
    return lax.dot_general(
        inputs, matrix, (((1,), (1,)), ((), ())), preferred_element_type=jnp.float32
    )


def swiglu_rows(inputs, gate_matrix, up_matrix, down_matrix):
    hidden = (
        jax.nn.silu(contract_rows(inputs, gate_matrix)) * contract_rows(inputs, up_matrix)
    ).astype(jnp.bfloat16)
    return jnp.dot(hidden, down_matrix, preferred_element_type=jnp.float32)


def dispatch_body(
    tokens,
    routes,
    route_weights,
    norm_gain,
    gate_trained,
    up_trained,
    down_trained,
    shared_gate_trained,
    shared_up_trained,
    shared_down_trained,
):
    gain_row = norm_gain[None, None, :]
    stacked = jnp.stack(
        [gate_trained * gain_row, up_trained * gain_row, down_trained], axis=1
    ).astype(jnp.bfloat16)
    halves = lax.all_to_all(
        lax.all_to_all(stacked[:, :, :, None, :], "fs", split_axis=0, concat_axis=2, tiled=True),
        "tp",
        split_axis=0,
        concat_axis=3,
        tiled=True,
    )
    owned = lax.all_gather(halves[:, :, :, None], "gr", axis=3, tiled=True)
    owned = owned.reshape(owned.shape[0], 3, owned.shape[2], -1)
    expert_gate = owned[:, 0]
    expert_up = owned[:, 1]
    expert_down = owned[:, 2]
    shared_gain = norm_gain[None, :]
    shared_stack = jnp.stack(
        [shared_gate_trained * shared_gain, shared_up_trained * shared_gain, shared_down_trained],
        axis=0,
    ).astype(jnp.bfloat16)
    shared_whole = lax.all_gather(shared_stack, ("gr", "tp"), axis=2, tiled=True)
    shared_gate = shared_whole[0]
    shared_up = shared_whole[1]
    shared_down = shared_whole[2]
    values = tokens.astype(jnp.float32)
    normed = (
        values * lax.rsqrt(jnp.mean(values * values, axis=1, keepdims=True) + epsilon)
    ).astype(jnp.bfloat16)
    row_count, features = normed.shape
    per_token = routes.shape[1]
    shared_out = swiglu_rows(
        normed,
        lax.all_gather(shared_gate, "fs", axis=0, tiled=True),
        lax.all_gather(shared_up, "fs", axis=0, tiled=True),
        lax.all_gather(shared_down, "fs", axis=0, tiled=True),
    )
    experts = lax.axis_size("fs") * lax.axis_size("tp")
    capacity = max(2, 3 * row_count * per_token // (2 * experts))
    chosen = routes.reshape(-1)
    onehot = (chosen[:, None] == jnp.arange(experts, dtype=jnp.int32)[None, :]).astype(jnp.int32)
    position = jnp.sum((jnp.cumsum(onehot, axis=0) - onehot) * onehot, axis=1)
    target = chosen * capacity + position
    source = (
        jnp.full((experts * capacity,), row_count, jnp.int32)
        .at[target]
        .set(jnp.arange(row_count * per_token, dtype=jnp.int32) // per_token)
    )
    padded = jnp.concatenate([normed, jnp.zeros((1, features), jnp.bfloat16)], axis=0)
    outgoing = padded[source].reshape(experts, capacity, features)
    arrived = lax.all_to_all(outgoing, ("fs", "tp"), split_axis=0, concat_axis=0, tiled=True)
    item_count = arrived.shape[1]
    result = swiglu_rows(
        arrived.reshape(-1, features), expert_gate[0], expert_up[0], expert_down[0]
    )
    result = result.astype(jnp.bfloat16).reshape(experts, item_count, features)
    returned = lax.all_to_all(result, ("fs", "tp"), split_axis=0, concat_axis=0, tiled=True)
    picked = returned.reshape(experts * capacity, features)[target].astype(jnp.float32)
    picked = picked.reshape(row_count, per_token, features)
    routed = jnp.sum(picked * route_weights[:, :, None], axis=1)
    combined = (routed + shared_out).astype(jnp.bfloat16)
    return (combined, expert_gate, expert_up, expert_down, shared_gate, shared_up, shared_down)


class Both:
    def __init__(self, *copies):
        self.copies = copies

    def start(self):
        for copy in self.copies:
            copy.start()

    def wait_recv(self):
        for copy in self.copies:
            copy.wait_recv()

    def wait_send(self):
        for copy in self.copies:
            copy.wait_send()


def exchange_kernel(
    n,
    tokens_hbm,
    routes_hbm,
    route_weights_hbm,
    gain_hbm,
    gate_hbm,
    up_hbm,
    down_hbm,
    shared_gate_hbm,
    shared_up_hbm,
    shared_down_hbm,
    combined_ref,
    owned,
    shared,
    weights,
    rows,
    table,
    select,
    tokens_ref,
    routes_ref,
    route_weights_ref,
    gain_ref,
    shared_stage,
    stage,
    pieces,
    guests,
    shared_mine,
    parts,
    pair_in,
    sums,
    side_in,
    mate_in,
    sums_in,
    local_sem,
    slice_out_sem,
    slice_sem,
    piece_sem,
    guest_out_sem,
    guest_sem,
    guest_on_sem,
    weight_sem,
    column_out_sem,
    column_sem,
    shared_out_sem,
    shared_sem,
    row_out_sem,
    row_side_sem,
    row_back_sem,
    row_sem,
    mix_out_sem,
    mix_back_sem,
    mix_sem,
    row_pair_out_sem,
    row_pair_sem,
    part_sem,
    part_recv_sem,
    side_sem,
    side_recv_sem,
    sum_sem,
    mate_sem,
    sum_recv_sem,
    stage_sem,
    input_sem,
):
    gr, fs, tp = lax.axis_index("gr"), lax.axis_index("fs"), lax.axis_index("tp")
    other = 1 - tp
    across = (1 - gr, fs, tp)
    across_twin = (1 - gr, fs, other)
    twin = (gr, fs, other)
    expert = fs * 2 + tp
    width = pieces.shape[2]
    hidden_piece = pieces.shape[1] // (2 * n)
    hidden = n * hidden_piece
    shared_piece = shared_mine.shape[1]
    extra = shared_piece // 2
    features = 4 * width
    row_count = tokens_ref.shape[0]
    depth = n // 2
    outer, inner = lax.div(fs, 2), lax.rem(fs, 2)
    beside = (gr, outer * 2 + 1 - inner, tp)
    toward = jnp.where(outer < depth // 2, 1, -1)

    inputs_in = []
    for i, (source, target) in enumerate(
        (
            (tokens_hbm, tokens_ref),
            (routes_hbm, routes_ref),
            (route_weights_hbm, route_weights_ref),
            (gain_hbm, gain_ref),
            (shared_gate_hbm, shared_stage.at[0]),
            (shared_up_hbm, shared_stage.at[1]),
            (shared_down_hbm, shared_stage.at[2]),
        )
    ):
        inputs_in.append(pltpu.make_async_copy(source, target, input_sem.at[i]))
        inputs_in[i].start()
    barrier = pltpu.get_barrier_semaphore()
    for device in (across, across_twin, twin):
        pl.semaphore_signal(barrier, inc=1, device_id=device, device_id_type=MESH)
    for k in range(1, n):
        for t in range(2):
            pl.semaphore_signal(
                barrier, inc=1, device_id=(gr, lax.rem(fs + k, n), t), device_id_type=MESH
            )

    own_start = pl.multiple_of(expert * row_count, row_count)
    few = 16
    inputs_in[0].wait()
    staged = {}
    for t in (0, 1):
        for j, ref in enumerate((gate_hbm, up_hbm, down_hbm)):
            part = pl.ds(t * hidden, hidden)
            staged[j, t] = pltpu.make_async_copy(ref.at[part], stage.at[j, part], stage_sem.at[j, t])
            staged[j, t].start()

    @pl.loop(0, row_count // few)
    def _(i):
        at = pl.multiple_of(i * few, few)
        values = tokens_ref[pl.ds(at, few), :].astype(jnp.float32)
        mean = jnp.mean(values * values, axis=1, keepdims=True)
        normed = (values * lax.rsqrt(mean + epsilon)).astype(jnp.bfloat16)
        rows[pl.ds(own_start + at, few), :] = normed

    for copy in inputs_in[1:]:
        copy.wait()
    number = lax.broadcasted_iota(jnp.int32, (2 * n, row_count), 0)
    factors = jnp.zeros(number.shape, jnp.float32)
    for k in range(routes_ref.shape[0]):
        named = routes_ref[k : k + 1, :] == number
        factors = factors + jnp.where(named, route_weights_ref[k : k + 1, :], 0.0)
    high = factors.astype(jnp.bfloat16).astype(jnp.float32)
    both = jnp.concatenate([high, factors - high], axis=0)
    table[expert] = both.astype(jnp.bfloat16)

    pl.semaphore_wait(barrier, 2 * n + 1)

    def remote(src, dst, send, recv, device):
        return pltpu.make_async_remote_copy(
            src_ref=src,
            dst_ref=dst,
            send_sem=send,
            recv_sem=recv,
            device_id=device,
            device_id_type=MESH,
        )

    def columns(g, t):
        return pl.ds(pl.multiple_of((g * 2 + t) * width, width), width)

    def piece(e):
        return pieces.at[:, pl.ds(pl.multiple_of(e * hidden_piece, 16), hidden_piece), :]

    def portion(t):
        return pieces.at[:, pl.ds(pl.multiple_of(t * hidden, 16), hidden), :]

    def sliced(g, t):
        return weights.at[:, pl.ds(0, hidden), columns(g, t)]

    def slab(source, span):
        start = pl.multiple_of(source * hidden_piece, 16)
        return owned.at[:, pl.ds(start, hidden_piece), span]

    def row_block(source, t):
        start = pl.multiple_of((source * 2 + t) * row_count, row_count)
        return rows.at[pl.ds(start, row_count)]

    late = row_count * 3 // 8
    early = row_count - late

    def row_early(source):
        start = pl.multiple_of((source * 2 + tp) * row_count, row_count)
        return rows.at[pl.ds(start, early)]

    def row_late(source):
        start = pl.multiple_of((source * 2 + tp) * row_count, row_count)
        return rows.at[pl.ds(pl.multiple_of(start + early, 16), late)]

    def nearby(k):
        place = lax.rem(outer + toward * lax.div(k, 2) + depth, depth)
        return place * 2 + jnp.where(lax.rem(k, 2) == 0, inner, 1 - inner)

    half = pl.ds(pl.multiple_of(gr * 2 * width, width), 2 * width)
    far_half = pl.ds(pl.multiple_of((1 - gr) * 2 * width, width), 2 * width)

    def slice_send(index, t, device):
        return remote(
            portion(t), sliced(gr, tp), slice_out_sem.at[index], slice_sem.at[index], device
        )

    def piece_send(d, t):
        return remote(
            piece(d * 2 + t),
            slab(fs, columns(gr, tp)),
            piece_sem.at[d, t],
            weight_sem.at[fs, tp],
            (gr, d, t),
        )

    pair = 2 * hidden_piece

    low = outer < depth // 2
    near = jnp.where(low, 1, 2 * depth - 3) - outer
    at_end = (outer == 0) | (outer == depth - 1)

    def direct(place, t):
        return False

    def unless(condition, action):
        if condition is False:
            action()
        else:
            pl.when(jnp.logical_not(condition))(action)

    def guest_send(place, t):
        e = (place * 2 + 1 - inner) * 2 + t
        spot = pl.ds(place * pair + t * hidden_piece, hidden_piece)
        return remote(
            piece(e),
            guests.at[:, spot, :],
            guest_out_sem.at[place, t],
            guest_sem.at[place, t],
            beside,
        )

    fs_beside = outer * 2 + 1 - inner

    def guest(place, t):
        start = pl.multiple_of(place * pair + t * hidden_piece, 16)
        return guests.at[:, pl.ds(start, hidden_piece), :]

    def guest_onward(place, t):
        return remote(
            guest(place, t),
            slab(fs_beside, columns(gr, tp)),
            guest_on_sem.at[place, t],
            weight_sem.at[fs_beside, tp],
            (gr, place * 2 + inner, t),
        )

    guest_local = pltpu.make_async_copy(
        guest(outer, tp), slab(fs_beside, columns(gr, tp)), local_sem.at[0]
    )

    def column_send(source):
        return remote(
            slab(source, half),
            slab(source, half),
            column_out_sem.at[source],
            column_sem.at[source],
            across,
        )

    def with_table(block, source, t, send, recv, device):
        entry = table.at[source * 2 + t]
        return Both(
            remote(block, block, send.at[0], recv.at[0], device),
            remote(entry, entry, send.at[1], recv.at[1], device),
        )

    def row_move(source, send, recv, device):
        return with_table(row_block(source, tp), source, tp, send, recv, device)

    def row_onward(source, step):
        return row_move(
            source,
            row_out_sem.at[source],
            row_sem.at[source],
            (gr, (outer + step) * 2 + inner, tp),
        )

    def row_beside(source, distance):
        block = row_early(source) if distance < depth - 1 else row_block(source, tp)
        return with_table(
            block, source, tp, row_side_sem.at[lax.div(source, 2)], row_sem.at[source], beside
        )

    def mixed(place, send, step):
        block = row_late(place * 2 + 1 - inner)
        device = (gr, (outer + step) * 2 + inner, tp)
        return remote(block, block, send, mix_sem.at[place], device)

    mix_up = mixed(outer, mix_out_sem.at[outer], 1)
    mix_back = mixed(outer, mix_back_sem.at[0], -1)

    def row_relay(source):
        return row_move(source, row_pair_out_sem.at[source], row_pair_sem.at[source], twin)

    own_up = row_move(fs, row_out_sem.at[fs], row_sem.at[fs], (gr, (outer + 1) * 2 + inner, tp))
    own_back = row_move(fs, row_back_sem.at[0], row_sem.at[fs], (gr, (outer - 1) * 2 + inner, tp))
    own_beside = row_move(fs, row_side_sem.at[outer], row_sem.at[fs], beside)
    own_relay = row_move(fs, row_pair_out_sem.at[fs], row_pair_sem.at[fs], twin)

    def at_distance(distance, action):
        for step in (-1, 1):
            place = outer - step * distance

            @pl.when((place >= 0) & (place < depth))
            def _():
                action(place, step, distance)

    def onward_exists(step):
        return (outer + step >= 0) & (outer + step < depth)

    @pl.when(outer < depth - 1)
    def _():
        own_up.start()

    @pl.when(outer > 0)
    def _():
        own_back.start()

    own_beside.start()
    own_relay.start()
    gain = gain_ref[...]
    for j in range(3):
        value = shared_stage[j] if j == 2 else shared_stage[j] * gain
        shared_mine[j] = value.astype(jnp.bfloat16)
    for t in (0, 1):
        for j in range(3):
            staged[j, t].wait()

            @pl.loop(0, n)
            def _(i):
                at = pl.ds(pl.multiple_of((t * n + i) * hidden_piece, hidden_piece), hidden_piece)
                value = stage[j, at, :] if j == 2 else stage[j, at, :] * gain_ref[...]
                pieces[j, at, :] = value.astype(jnp.bfloat16)

    lane = lax.broadcasted_iota(jnp.int32, select.shape, 0)
    unit = lax.broadcasted_iota(jnp.int32, select.shape, 1)
    first = (jnp.where(lane < 2 * n, lane, lane - 2 * n) - tp * n) * hidden_piece
    inside = (unit >= first) & (unit < first + hidden_piece) & (unit < hidden)
    select[...] = jnp.where(inside, 1.0, 0.0).astype(select.dtype)
    shared_far = remote(
        shared_mine, shared.at[:, :, columns(gr, tp)], shared_out_sem.at[0], shared_sem.at[0], across
    )
    shared_far.start()
    slice_far = slice_send(0, tp, across)
    slice_cross = slice_send(1, other, across_twin)
    slice_twin = slice_send(2, other, twin)
    slice_far.start()
    slice_cross.start()
    slice_twin.start()
    shared_twin = remote(
        shared_mine, shared.at[:, :, columns(gr, tp)], shared_out_sem.at[1], shared_sem.at[1], twin
    )
    shared_twin.start()
    twin_piece = piece_send(fs, other)
    twin_piece.start()

    def ship(places):
        for place in places:

            @pl.when(place != outer)
            def _():
                piece_send(place * 2 + inner, 0).start()
                piece_send(place * 2 + inner, 1).start()

    own_slice = pltpu.make_async_copy(portion(tp), sliced(gr, tp), local_sem.at[1])
    own_piece = pltpu.make_async_copy(piece(expert), slab(fs, columns(gr, tp)), local_sem.at[2])
    own_shared = pltpu.make_async_copy(
        shared_mine, shared.at[:, :, columns(gr, tp)], local_sem.at[3]
    )
    locals_ = (own_slice, own_piece, own_shared)
    for copy in locals_:
        copy.start()

    def take_rows(source):
        row_move(source, row_out_sem.at[source], row_sem.at[source], twin).wait_recv()

    def arrive(place, step, distance):
        source = place * 2 + inner
        take_rows(source)

        @pl.when(onward_exists(step))
        def _():
            row_onward(source, step).start()

        row_beside(source, distance).start()
        row_relay(source).start()

    def arrive_mixed(place, step, distance):
        mixed(place, mix_out_sem.at[place], step).wait_recv()
        if distance < depth - 2:

            @pl.when(onward_exists(step))
            def _():
                mixed(place, mix_out_sem.at[place], step).start()

    def arrive_beside(place, step, distance):
        source = place * 2 + 1 - inner
        row_beside(source, distance).wait_recv()
        row_relay(source).start()

    at_distance(1, arrive)
    take_rows(outer * 2 + 1 - inner)

    @pl.when(outer < depth - 1)
    def _():
        mix_up.start()

    @pl.when(outer > 0)
    def _():
        mix_back.start()

    row_relay(outer * 2 + 1 - inner).start()
    for place in range(depth):
        for t in range(2):
            unless(direct(place, t), guest_send(place, t).start)
    for copy in locals_:
        copy.wait()
    far_columns = shared.at[:, :, columns(1 - gr, tp)]
    remote(shared_mine, far_columns, shared_out_sem.at[0], shared_sem.at[0], across).wait_recv()
    shared_relay = remote(far_columns, far_columns, shared_out_sem.at[2], shared_sem.at[2], twin)
    shared_relay.start()
    at_distance(2, arrive)
    ship(range(1, depth - 1))

    at_distance(1, arrive_mixed)
    at_distance(1, arrive_beside)
    at_distance(3, arrive)
    at_distance(2, arrive_mixed)
    ship((0, depth - 1))

    for place in range(depth):
        for t in range(2):

            def onward(place=place, t=t):
                guest_send(place, t).wait_recv()

                @pl.when(place != outer)
                def _():
                    guest_onward(place, t).start()

            unless(direct(place, t), onward)

    guest_onward(outer, other).start()
    guest_local.start()
    guest_local.wait()

    def take_twin_piece(source, t):
        remote(
            piece(0),
            slab(source, columns(gr, t)),
            piece_sem.at[fs, other],
            weight_sem.at[source, t],
            twin,
        ).wait_recv()

    take_twin_piece(fs, other)
    column_send(fs).start()
    take_twin_piece(fs_beside, other)
    column_send(fs_beside).start()

    remote(
        shared_mine, shared.at[:, :, columns(gr, other)], shared_out_sem.at[1], shared_sem.at[1], twin
    ).wait_recv()
    last_columns = shared.at[:, :, columns(1 - gr, other)]
    remote(shared_mine, last_columns, shared_out_sem.at[2], shared_sem.at[2], twin).wait_recv()
    tail = pltpu.make_async_copy(
        shared.at[:, pl.ds(pl.multiple_of(tp * extra, extra), extra), :],
        weights.at[:, pl.ds(hidden, extra), :],
        local_sem.at[4],
    )
    tail.start()
    tail.wait()
    remote(portion(tp), sliced(gr, other), slice_out_sem.at[2], slice_sem.at[2], twin).wait_recv()
    remote(portion(tp), sliced(1 - gr, tp), slice_out_sem.at[0], slice_sem.at[0], across).wait_recv()
    remote(
        portion(tp), sliced(1 - gr, other), slice_out_sem.at[1], slice_sem.at[1], across
    ).wait_recv()

    def part_send(k):
        return remote(
            parts.at[k, pl.ds(pl.multiple_of(other * row_count, row_count), row_count), :],
            pair_in.at[k],
            part_sem.at[k],
            part_recv_sem.at[k],
            twin,
        )

    def place_of(j):
        far = jnp.where(low, depth // 2 + j, depth // 2 - 1 - j)
        return jnp.where(j < depth // 2, far, jnp.where(j == depth - 1, outer, near))

    steps = 2
    span_rows = row_count // steps

    def share(h):
        return pl.ds(h * span_rows, span_rows)

    def side_send(j, h):
        return remote(
            sums.at[2 * j, share(h)],
            side_in.at[j, share(h)],
            side_sem.at[j, h],
            side_recv_sem.at[j, h],
            beside,
        )

    def mate_send(j, h):
        return remote(
            sums.at[2 * j + 1, share(h)],
            mate_in.at[j, share(h)],
            sum_sem.at[j, h],
            mate_sem.at[j, h],
            (gr, near * 2 + inner, tp),
        )

    def sum_send(j, h):
        slot = 1 if j < depth // 2 else 0
        return remote(
            sums.at[2 * j + 1, share(h)],
            sums_in.at[slot, share(h)],
            sum_sem.at[j, h],
            sum_recv_sem.at[slot, h],
            (gr, place_of(j) * 2 + inner, tp),
        )

    chunk = 32

    def add_pair(k, h):
        @pl.loop(0, span_rows // chunk)
        def _(i):
            at = pl.multiple_of(h * span_rows + i * chunk, chunk)
            mine = pl.multiple_of(tp * row_count + at, chunk)
            value = parts[k, pl.ds(mine, chunk), :].astype(jnp.float32)
            value = value + pair_in[k, pl.ds(at, chunk), :].astype(jnp.float32)
            sums[k, pl.ds(at, chunk), :] = value.astype(jnp.bfloat16)

    def await_both(j, h):
        if h == 0:
            part_send(2 * j + 1).wait_recv()
        side_send(j, h).wait_recv()

    def add_both(j, h, mate):
        k = 2 * j + 1

        @pl.loop(0, span_rows // chunk)
        def _(i):
            at = pl.multiple_of(h * span_rows + i * chunk, chunk)
            mine = pl.multiple_of(tp * row_count + at, chunk)
            value = parts[k, pl.ds(mine, chunk), :].astype(jnp.float32)
            value = value + pair_in[k, pl.ds(at, chunk), :].astype(jnp.float32)
            value = value + side_in[j, pl.ds(at, chunk), :].astype(jnp.float32)
            if mate:
                value = value + mate_in[j, pl.ds(at, chunk), :].astype(jnp.float32)
            sums[k, pl.ds(at, chunk), :] = value.astype(jnp.bfloat16)

    def take_weights(source):
        take_twin_piece(source, 0)
        take_twin_piece(source, 1)
        column_send(source).start()

    def pass_far(j, h):
        await_both(j, h)

        @pl.when(at_end)
        def _():
            add_both(j, h, False)
            mate_send(j, h).start()

        @pl.when(jnp.logical_not(at_end))
        def _():
            mate_send(j, h).wait_recv()
            add_both(j, h, True)
            sum_send(j, h).start()

    def pass_near(j):
        for h in range(steps):
            await_both(j, h)
            add_both(j, h, False)
            sum_send(j, h).start()

    @pl.loop(0, n)
    def _(k):
        turn = lax.div(k, 2)
        swapped = jnp.logical_not(at_end) & (turn > 0) & (turn < depth - 1)
        j = jnp.where(swapped, depth - 1 - turn, turn)
        item = 2 * j + lax.rem(k, 2)
        d = place_of(j) * 2 + jnp.where(lax.rem(k, 2) == 0, 1 - inner, inner)

        @pl.when(k == jnp.where(at_end, 0, 4))
        def _():
            at_distance(2, arrive_beside)

        @pl.when(k == 2)
        def _():
            at_distance(3, arrive_beside)

        with_table(
            row_block(d, other), d, other, row_pair_out_sem.at[d], row_pair_sem.at[d], twin
        ).wait_recv()
        block = pl.ds(pl.multiple_of(d * 2 * row_count, 2 * row_count), 2 * row_count)
        inputs = rows[block, :]
        entries = [table[d * 2 + t].astype(jnp.float32).T.astype(jnp.bfloat16) for t in range(2)]
        scale = jnp.dot(
            jnp.concatenate(entries, axis=0), select[...], preferred_element_type=jnp.float32
        )
        gate = contract_rows(inputs, weights[0])
        up = contract_rows(inputs, weights[1])
        position = lax.broadcasted_iota(jnp.int32, gate.shape, 1)
        scale = jnp.where(position < hidden, scale, 1.0)
        units = (gate / (1.0 + jnp.exp(-gate)) * up * scale).astype(jnp.bfloat16)
        for c in range(4):
            span = pl.ds(c * width, width)
            parts[item, :, span] = jnp.dot(
                units, weights[2, :, span], preferred_element_type=jnp.float32
            ).astype(jnp.bfloat16)
        part_send(item).start()

        @pl.when(lax.rem(k, 2) == 1)
        def _():
            part_send(item - 1).wait_recv()
            for h in range(steps):
                add_pair(item - 1, h)
                side_send(j, h).start()

        @pl.when((k > 1) & (k <= depth))
        def _():
            take_weights(nearby(2 * k - 2))

        for h in range(steps):

            @pl.when((k == n - 5 + 2 * h // steps) & at_end)
            def _():
                pass_far(0, h)

        @pl.when((k > depth) & (k < n - 1) & at_end)
        def _():
            take_weights(nearby(2 * (k - depth) + 1))


    @pl.when(jnp.logical_not(at_end))
    def _():
        take_weights(nearby(3))
        pass_near(2)
        for h in range(steps):
            pass_far(0, h)
        for i in range(2, depth):
            take_weights(nearby(2 * i + 1))

    for h in range(steps):
        pass_far(1, h)

    @pl.when(at_end)
    def _():
        take_weights(nearby(n - 1))
        pass_near(2)


    for k in range(n):
        source = nearby(k)
        remote(
            slab(source, far_half),
            slab(source, far_half),
            column_out_sem.at[source],
            column_sem.at[source],
            across,
        ).wait_recv()

    for h in range(steps):
        await_both(depth - 1, h)
        add_both(depth - 1, h, False)
    for h in range(steps):
        for j in range(2):
            remote(
                sums.at[0, share(h)],
                sums_in.at[j, share(h)],
                sum_sem.at[0, 0],
                sum_recv_sem.at[j, h],
                twin,
            ).wait_recv()

        @pl.loop(0, span_rows // chunk)
        def _(i):
            at = pl.ds(pl.multiple_of(h * span_rows + i * chunk, chunk), chunk)
            total = sums[n - 1, at, :].astype(jnp.float32)
            for j in range(2):
                total = total + sums_in[j, at, :].astype(jnp.float32)
            combined_ref[at, :] = total.astype(jnp.bfloat16)

    @pl.when(outer < depth - 1)
    def _():
        own_up.wait_send()
        mix_up.wait_send()

    @pl.when(outer > 0)
    def _():
        own_back.wait_send()
        mix_back.wait_send()

    for copy in (
        own_beside,
        own_relay,
        shared_far,
        slice_far,
        slice_cross,
        slice_twin,
        shared_twin,
        twin_piece,
        shared_relay,
    ):
        copy.wait_send()

    def sent(place, step, distance):
        source = place * 2 + inner

        @pl.when(onward_exists(step))
        def _():
            row_onward(source, step).wait_send()
            if distance < depth - 2:
                mixed(place, mix_out_sem.at[place], step).wait_send()

        row_beside(source, distance).wait_send()

    for distance in range(1, depth):
        at_distance(distance, sent)
    column_send(fs).wait_send()
    for k in range(1, n):
        d = lax.rem(fs + k, n)
        column_send(d).wait_send()
        row_relay(d).wait_send()
    for place in range(depth):
        for t in range(2):

            def done(place=place, t=t):
                guest_send(place, t).wait_send()

                @pl.when(place != outer)
                def _():
                    guest_onward(place, t).wait_send()

            unless(direct(place, t), done)

            @pl.when(place != outer)
            def _():
                piece_send(place * 2 + inner, t).wait_send()

    guest_onward(outer, other).wait_send()

    for k in range(n):
        part_send(k).wait_send()
    for h in range(steps):
        for j in range(depth):
            side_send(j, h).wait_send()
        for j in range(depth - 1):
            sum_send(j, h).wait_send()


def direct_body(
    tokens,
    routes,
    route_weights,
    norm_gain,
    gate_trained,
    up_trained,
    down_trained,
    shared_gate_trained,
    shared_up_trained,
    shared_down_trained,
):
    n = lax.axis_size("fs")
    experts, hidden_piece, width = gate_trained.shape
    row_count, features = tokens.shape
    shared_piece = shared_gate_trained.shape[0]
    stacked = (experts * hidden_piece, width)
    hidden = n * hidden_piece
    hidden_all = hidden + shared_piece // 2
    vmem = pl.BlockSpec(memory_space=pltpu.VMEM)
    hbm = pl.BlockSpec(memory_space=pltpu.HBM)
    kind = jnp.bfloat16
    DMA = pltpu.SemaphoreType.DMA
    combined, owned, shared = pl.pallas_call(
        functools.partial(exchange_kernel, n),
        out_shape=(
            jax.ShapeDtypeStruct((row_count, features), kind),
            jax.ShapeDtypeStruct((3, hidden, features), kind),
            jax.ShapeDtypeStruct((3, shared_piece, features), kind),
        ),
        in_specs=[hbm] * 10,
        out_specs=(vmem,) * 3,
        scratch_shapes=[
            pltpu.VMEM((3, hidden_all, features), kind),
            pltpu.VMEM((experts * row_count, features), kind),
            pltpu.VMEM((experts, 2 * experts, row_count), kind),
            pltpu.VMEM((2 * experts, hidden_all), kind),
            pltpu.VMEM((row_count, features), kind),
            pltpu.VMEM(routes.shape[::-1], jnp.int32),
            pltpu.VMEM(routes.shape[::-1], jnp.float32),
            pltpu.VMEM((1, width), jnp.float32),
            pltpu.VMEM((3, shared_piece, width), jnp.float32),
            pltpu.VMEM((3,) + stacked, jnp.float32),
            pltpu.VMEM((3,) + stacked, kind),
            pltpu.VMEM((3, n * hidden_piece, width), kind),
            pltpu.VMEM((3, shared_piece, width), kind),
            pltpu.VMEM((n, 2 * row_count, features), kind),
            pltpu.VMEM((n, row_count, features), kind),
            pltpu.VMEM((n, row_count, features), kind),
            pltpu.VMEM((n // 2, row_count, features), kind),
            pltpu.VMEM((n // 4, row_count, features), kind),
            pltpu.VMEM((2, row_count, features), kind),
            DMA((5,)),
            DMA((3,)),
            DMA((3,)),
            DMA((n, 2)),
            DMA((n // 2, 2)),
            DMA((n // 2, 2)),
            DMA((n // 2, 2)),
            DMA((n, 2)),
            DMA((n,)),
            DMA((n,)),
            DMA((3,)),
            DMA((3,)),
            DMA((n, 2)),
            DMA((n // 2, 2)),
            DMA((1, 2)),
            DMA((n, 2)),
            DMA((n // 2,)),
            DMA((1,)),
            DMA((n // 2,)),
            DMA((n, 2)),
            DMA((n, 2)),
            DMA((n,)),
            DMA((n,)),
            DMA((n // 2, 2)),
            DMA((n // 2, 2)),
            DMA((n // 2 - 1, 2)),
            DMA((n // 4, 2)),
            DMA((2, 2)),
            DMA((3, 2)),
            DMA((7,)),
        ],
        compiler_params=pltpu.CompilerParams(
            collective_id=0, has_side_effects=True, vmem_limit_bytes=48 * 1024 * 1024
        ),
    )(*[
        pltpu.with_memory_space_constraint(array, pltpu.HBM)
        for array in (
            tokens,
            routes.T,
            route_weights.T,
            norm_gain[None, :],
            gate_trained.reshape(stacked),
            up_trained.reshape(stacked),
            down_trained.reshape(stacked),
            shared_gate_trained,
            shared_up_trained,
            shared_down_trained,
        )
    ])
    return settle(combined, owned, shared)


def settle_kernel(combined_ref, owned_ref, shared_ref, combined_out, *refs):
    sems = refs[-1]
    copies = [pltpu.make_async_copy(combined_ref, combined_out, sems.at[6])]
    for j in range(3):
        copies.append(pltpu.make_async_copy(owned_ref.at[j], refs[j].at[0], sems.at[j]))
        copies.append(pltpu.make_async_copy(shared_ref.at[j], refs[3 + j], sems.at[3 + j]))
    for copy in copies:
        copy.start()
    for copy in copies:
        copy.wait()


def settle(combined, owned, shared):
    expert_shape = jax.ShapeDtypeStruct((1,) + owned.shape[1:], owned.dtype)
    shared_shape = jax.ShapeDtypeStruct(shared.shape[1:], shared.dtype)
    return pl.pallas_call(
        settle_kernel,
        out_shape=(jax.ShapeDtypeStruct(combined.shape, combined.dtype),)
        + (expert_shape,) * 3
        + (shared_shape,) * 3,
        in_specs=[pl.BlockSpec(memory_space=pltpu.VMEM)] * 3,
        out_specs=(pl.BlockSpec(memory_space=pltpu.HBM),) * 7,
        scratch_shapes=[pltpu.SemaphoreType.DMA((7,))],
        compiler_params=pltpu.CompilerParams(vmem_limit_bytes=8 * 1024 * 1024),
    )(combined, owned, shared)


def body(*arguments):
    experts = lax.axis_size("fs") * lax.axis_size("tp")
    per_token = arguments[1].shape[1]
    pairs = lax.axis_size("gr") == 2 and lax.axis_size("tp") == 2
    if pairs and lax.axis_size("fs") == 8 and experts <= min(2 * per_token, LANES // 2):
        return direct_body(*arguments)
    return dispatch_body(*arguments)


def solution(mesh):
    in_specs = (
        P(("gr", "fs", "tp"), None),
        P(("gr", "fs", "tp"), None),
        P(("gr", "fs", "tp"), None),
        P(("gr", "tp")),
        P(None, "fs", ("gr", "tp")),
        P(None, "fs", ("gr", "tp")),
        P(None, "fs", ("gr", "tp")),
        P("fs", ("gr", "tp")),
        P("fs", ("gr", "tp")),
        P("fs", ("gr", "tp")),
    )
    out_specs = (
        P(("gr", "fs", "tp"), None),
        P(("fs", "tp"), None, None),
        P(("fs", "tp"), None, None),
        P(("fs", "tp"), None, None),
        P("fs", None),
        P("fs", None),
        P("fs", None),
    )
    return jax.shard_map(body, mesh=mesh, in_specs=in_specs, out_specs=out_specs, check_vma=False)
```
